256 devices in a mesh: sp: 32 (over z, y), fs: 4 (over x), tp: 2 (over core).
Axes of the slice: x: 4, y: 4, z: 8, core: 2. Of those that a mesh axis runs over, the one named last changes fastest.
Arguments:
- hidden_in: bfloat16 [4, 8192, 2048], P('fs', 'sp', 'tp'), may hold values from -6 to 6
- sb_query_w: bfloat16 [2048, 1024], P('fs', 'tp'), may hold values from -0.21875 to 0.21875
- sb_key_w: bfloat16 [2048, 1024], P('fs', 'tp'), may hold values from -0.21875 to 0.21875
- sb_value_w: bfloat16 [2048, 1024], P('fs', 'tp'), may hold values from -0.125 to 0.125
- sb_offset: float32 [16], P('tp'), may hold values from -16 to -6
- delta_query_w: bfloat16 [2048, 1024], P('fs', 'tp'), may hold values from -0.125 to 0.125
- delta_key_w: bfloat16 [2048, 1024], P('fs', 'tp'), may hold values from -0.125 to 0.125
- delta_value_w: bfloat16 [2048, 1024], P('fs', 'tp'), may hold values from -0.125 to 0.125
- decay_w: bfloat16 [2048, 8], P(None, 'tp'), may hold values from -0.125 to 0.125
- write_w: bfloat16 [2048, 8], P(None, 'tp'), may hold values from -0.125 to 0.125
- write_bias: float32 [8], P('tp'), may hold values from -7 to 1.5
- decay_log_scale: float32 [8], P('tp'), may hold values from -14 to -3
- decay_shift: float32 [4, 8, 8192], P('fs', 'tp', 'sp'), may hold values from -3 to 0
- head_gain: float32 [128], replicated, may hold values from 0.1 to 1.9
- sb_out_w: bfloat16 [1024, 2048], P('tp'), may hold values from -0.125 to 0.125
- delta_out_w: bfloat16 [1024, 2048], P('tp'), may hold values from -0.125 to 0.125
Outputs:
- mixed_out: bfloat16 [4, 8192, 2048], P('fs', ('sp', 'tp'))
The draws below stay inside these ranges and needn't reach their ends.
All inputs are finite; a program needn't handle non-finite values.
Results may differ from the reference program's by a relative error of at most 0.015.
Values may be sent and summed in bfloat16 or wider, within the bound.
No kernel may reach another device: no remote copies, remote signals or barrier semaphores. Data moves between devices by JAX's collectives and lax.ppermute only.
A program may use at most 128 MiB of HBM per device.

```python
import jax
import jax.numpy as jnp
from jax import lax

D = 2048
SB_HEADS = 16
SB_DIM = 64
GDN_HEADS = 8
GDN_DIM = 128
BLOCK = 64
TOK_DEV = 256
LEN = 8192
SEQS = 4
N_TP = 2


def head_kinds(key, fast_share):
    return jax.random.uniform(jax.random.fold_in(key, 71), (GDN_HEADS,), jnp.float32) < fast_share


def draw_sb_offset(key, part):
    reach_term = jax.random.uniform(key, (SB_HEADS,), jnp.float32, -1.0, 2.5)
    return reach_term - jnp.log(jnp.float32(LEN)) - 4.5


def draw_write_bias(key, part):
    fast_share = 0.5
    chosen = head_kinds(key, fast_share)
    strong_term = jax.random.uniform(jax.random.fold_in(key, 5), (GDN_HEADS,), jnp.float32, -1.0, 1.5)
    faint_summand = jax.random.uniform(jax.random.fold_in(key, 6), (GDN_HEADS,), jnp.float32, -7.0, -5.5)
    return jnp.where(chosen, strong_term, faint_summand)


def draw_decay_log_scale(key, part):
    split_keys = jax.random.split(key, 3)
    fast_share = 0.5
    chosen = head_kinds(key, fast_share)
    fast_rate = jax.random.uniform(split_keys[1], (GDN_HEADS,), jnp.float32, 0.015, 0.04)
    slow_rate = jax.random.uniform(split_keys[2], (GDN_HEADS,), jnp.float32, 2e-06, 8e-06)
    return jnp.log(jnp.where(chosen, fast_rate, slow_rate))


def draw_decay_shift(key, part):
    split_keys = jax.random.split(key, 3)
    blocks_count = LEN // TOK_DEV
    minimal_level = 0.15
    highest = 1.2
    rates = jnp.exp(jax.random.uniform(split_keys[0], (SEQS, GDN_HEADS, blocks_count), jnp.float32, jnp.log(minimal_level), jnp.log(highest)))
    unweighted_result = jnp.repeat(rates, TOK_DEV, axis=2) * (-1.0 / LEN)
    destination_indices = jax.random.randint(split_keys[1], (SEQS, GDN_HEADS, 3), 0, LEN)
    forgetting_amounts = jnp.log(jax.random.uniform(split_keys[2], (SEQS, GDN_HEADS, 3), jnp.float32, 0.5, 0.8))
    cell_locations = jnp.arange(LEN, dtype=jnp.int32)
    storing_pulses = jnp.sum(jnp.where(cell_locations[None, None, None, :] == destination_indices[..., None], forgetting_amounts[..., None], 0.0), axis=2)
    return unweighted_result + storing_pulses


def shard_levels(own_key, dims, pieces, smallest, top_value):
    gain, own = 1.0, jax.random.fold_in(own_key, 6)
    for axis_at, blocks in pieces:
        heights = jnp.exp(jax.random.uniform(jax.random.fold_in(own, axis_at), (blocks,), jnp.float32, smallest / len(pieces), top_value / len(pieces)))
        gain = gain * jnp.repeat(heights, dims[axis_at] // blocks).reshape([-1 if axis == axis_at else 1 for axis in range(len(dims))])
    return gain


def gaussian(own_key, dims, scale, reach, shards=(), kind=jnp.bfloat16):
    drawn = jax.random.normal(own_key, dims, jnp.float32) * scale
    if len(shards) > 0:
        drawn = shard_levels(own_key, dims, shards, -0.22, 0.18) * drawn
    return jnp.clip(drawn, min=-reach, max=reach).astype(kind)


def setup_inputs(seed: int = 0) -> dict:
    streams_of = jax.random.split(jax.random.key(seed), 17)
    hidden_in = gaussian(streams_of[0], (SEQS, LEN, D), 1.0, 6.0, ((0, 4), (1, 32), (2, 2)))
    sb_query_w = gaussian(streams_of[1], (D, SB_HEADS * SB_DIM), (D // 3) ** -0.5, 0.21875, ((0, 4), (1, 2)))
    sb_key_w = gaussian(streams_of[2], (D, SB_HEADS * SB_DIM), (D // 3) ** -0.5, 0.21875, ((0, 4), (1, 2)))
    sb_value_w = gaussian(streams_of[3], (D, SB_HEADS * SB_DIM), D ** -0.5, 0.125, ((0, 4), (1, 2)))
    sb_offset = draw_sb_offset(jax.random.fold_in(streams_of[16], 71), 0)
    delta_query_w = gaussian(streams_of[5], (D, GDN_HEADS * GDN_DIM), D ** -0.5, 0.125, ((0, 4), (1, 2)))
    delta_key_w = gaussian(streams_of[6], (D, GDN_HEADS * GDN_DIM), D ** -0.5, 0.125, ((0, 4), (1, 2)))
    delta_value_w = gaussian(streams_of[7], (D, GDN_HEADS * GDN_DIM), D ** -0.5, 0.125, ((0, 4), (1, 2)))
    decay_w = gaussian(streams_of[8], (D, GDN_HEADS), D ** -0.5, 0.125, ((1, 2),))
    write_w = gaussian(streams_of[9], (D, GDN_HEADS), D ** -0.5, 0.125, ((1, 2),))
    write_bias = draw_write_bias(jax.random.fold_in(streams_of[16], 71), 0)
    decay_log_scale = draw_decay_log_scale(jax.random.fold_in(streams_of[16], 71), 0)
    decay_shift = draw_decay_shift(jax.random.fold_in(streams_of[16], 71), 0)
    head_gain = jnp.clip(1.0 + 0.18 * jax.random.normal(streams_of[13], (GDN_DIM,), jnp.float32), 0.1, 1.9)
    sb_out_w = gaussian(streams_of[14], (SB_HEADS * SB_DIM, D), (SB_HEADS * SB_DIM + GDN_HEADS * GDN_DIM) ** -0.5, 0.125, ((0, 2),))
    delta_out_w = gaussian(streams_of[15], (GDN_HEADS * GDN_DIM, D), (SB_HEADS * SB_DIM + GDN_HEADS * GDN_DIM) ** -0.5, 0.125, ((0, 2),))
    return dict(hidden_in=hidden_in, sb_query_w=sb_query_w, sb_key_w=sb_key_w, sb_value_w=sb_value_w, sb_offset=sb_offset, delta_query_w=delta_query_w, delta_key_w=delta_key_w, delta_value_w=delta_value_w, decay_w=decay_w, write_w=write_w, write_bias=write_bias, decay_log_scale=decay_log_scale, decay_shift=decay_shift, head_gain=head_gain, sb_out_w=sb_out_w, delta_out_w=delta_out_w)


EXACT_MATMUL = lax.Precision.HIGHEST
NORM_EPS = 1e-06

def unit_lower_inverse(strict_part):
    order_size = strict_part.shape[-1]
    powered = strict_part
    inverse = jnp.eye(order_size, dtype=strict_part.dtype) - strict_part
    for repeat_number in range(max(1, (order_size - 1).bit_length()) - 1):
        powered = jnp.einsum('...ij,...jk->...ik', powered, powered, precision=EXACT_MATMUL)
        inverse = inverse + jnp.einsum('...ij,...jk->...ik', inverse, powered, precision=EXACT_MATMUL)
    return inverse

def to_blocks(row_data, block_span):
    blocks_count = row_data.shape[0] // block_span
    shaped = row_data.reshape((blocks_count, block_span) + row_data.shape[1:])
    return jnp.swapaxes(shaped, 1, 2)

def from_blocks(blocked):
    swapped = jnp.swapaxes(blocked, 1, 2)
    return swapped.reshape((-1,) + swapped.shape[2:])

def unit_rows(vectors):
    return vectors * lax.rsqrt(lax.optimization_barrier(jnp.sum(vectors * vectors, axis=-1, keepdims=True)) + NORM_EPS)

def delta_inputs(query_proj, key_proj, value_proj, decay_pre, write_pre, write_bias, decay_log_scale, shift_rows, head_count, head_size):
    query_act = jax.nn.silu(query_proj.astype(jnp.float32)).reshape(-1, head_count, head_size)
    key_act = jax.nn.silu(key_proj.astype(jnp.float32)).reshape(-1, head_count, head_size)
    value_rows = jax.nn.silu(value_proj.astype(jnp.float32)).reshape(-1, head_count, head_size)
    queries = unit_rows(query_act) * head_size ** (-0.5)
    key_rows = unit_rows(key_act)
    log_decay = -jnp.exp(decay_log_scale) * jax.nn.softplus(decay_pre) + shift_rows
    strength = jax.nn.sigmoid(write_pre + write_bias)
    return (queries, key_rows, value_rows, log_decay, strength)

def delta_prepare(queries, key_rows, value_rows, log_decay, strength):
    block_span = queries.shape[2]
    cumulative = jnp.cumsum(log_decay, axis=-1)
    row_place = lax.broadcasted_iota(jnp.int32, (block_span, block_span), 0)
    col_place = lax.broadcasted_iota(jnp.int32, (block_span, block_span), 1)
    inclusive = col_place <= row_place
    strictly = col_place < row_place
    spread = cumulative[..., :, None] - cumulative[..., None, :]
    decay_table = jnp.where(inclusive, jnp.exp(jnp.where(inclusive, spread, 0.0)), 0.0)
    keys_beta = key_rows * strength[..., None]
    lower_part = jnp.where(strictly, jnp.einsum('nhik,nhjk->nhij', keys_beta, key_rows, precision=EXACT_MATMUL) * decay_table, 0.0)
    inverse = unit_lower_inverse(lower_part)
    growth = jnp.exp(cumulative)
    state_updates = jnp.einsum('nhij,nhjv->nhiv', inverse, value_rows * strength[..., None], precision=EXACT_MATMUL)
    erase_term = jnp.einsum('nhij,nhjk->nhik', inverse, keys_beta * growth[..., None], precision=EXACT_MATMUL)
    inside_block = jnp.einsum('nhik,nhjk->nhij', queries, key_rows, precision=EXACT_MATMUL) * decay_table
    boosted_query = queries * growth[..., None]
    damped_keys = key_rows * jnp.exp(cumulative[..., -1:] - cumulative)[..., None]
    decay_per_block = jnp.exp(cumulative[..., -1])
    return (state_updates, erase_term, inside_block, boosted_query, damped_keys, decay_per_block)

def delta_step(memory_state, inputs):
    state_updates, erase_term, inside_block, boosted_query, damped_keys, decay_per_block = inputs
    fixed_values = state_updates - jnp.einsum('mzq,mqc->mzc', erase_term, memory_state, precision=EXACT_MATMUL)
    produced_rows = jnp.einsum('mzq,mqc->mzc', boosted_query, memory_state, precision=EXACT_MATMUL) + jnp.einsum('efq,eqn->efn', inside_block, fixed_values, precision=EXACT_MATMUL)
    memory_state = memory_state * decay_per_block[:, None, None] + jnp.einsum('wam,waz->wmz', damped_keys, fixed_values, precision=EXACT_MATMUL)
    return (memory_state, produced_rows)

def stick_block(queries, key_rows, value_rows, query_place, key_place, offsets):
    scale_factor = queries.shape[-1] ** (-0.5)
    scores = jnp.einsum('qhd,khd->hqk', queries.astype(jnp.float32), key_rows.astype(jnp.float32)) * scale_factor + offsets[:, None, None]
    visible = key_place[None, :] < query_place[:, None]
    skipped = jnp.where(visible, jax.nn.log_sigmoid(-scores), 0.0)
    beyond = lax.cumsum(skipped, axis=2, reverse=True) - skipped
    weights = jnp.where(visible, jnp.exp(jax.nn.log_sigmoid(scores) + beyond), 0.0).astype(jnp.bfloat16)
    weights = lax.optimization_barrier(weights).astype(jnp.float32)
    partial_value = jnp.einsum('hqk,khd->qhd', weights, value_rows.astype(jnp.float32))
    return (partial_value, lax.optimization_barrier(jnp.sum(skipped, axis=2)).T)

def stick_combine(partials, totals):
    beyond = jnp.cumsum(totals[::-1], axis=0)[::-1] - totals
    return lax.optimization_barrier(jnp.sum(partials * jnp.exp(beyond)[..., None], axis=0))

def stick_sequence(queries, key_rows, value_rows, offsets):
    blocks_count = LEN // TOK_DEV
    query_blocks = queries.reshape((blocks_count, TOK_DEV) + queries.shape[1:])
    key_blocks = key_rows.reshape((blocks_count, TOK_DEV) + key_rows.shape[1:])
    value_blocks = value_rows.reshape((blocks_count, TOK_DEV) + value_rows.shape[1:])
    cell_locations = jnp.arange(LEN, dtype=jnp.int32).reshape(blocks_count, TOK_DEV)
    head_count = queries.shape[1]
    head_size = value_rows.shape[2]

    def per_query(query_index):

        def per_key(key_index):

            def active(unused_arg):
                return stick_block(query_blocks[query_index], key_blocks[key_index], value_blocks[key_index], cell_locations[query_index], cell_locations[key_index], offsets)

            def inactive(unused_arg):
                return (jnp.zeros((TOK_DEV, head_count, head_size), jnp.float32), jnp.zeros((TOK_DEV, head_count), jnp.float32))
            return lax.cond(key_index <= query_index, active, inactive, 0)
        partials, totals = lax.map(per_key, jnp.arange(blocks_count, dtype=jnp.int32))
        return stick_combine(partials, totals)
    gathered = lax.map(per_query, jnp.arange(blocks_count, dtype=jnp.int32))
    return gathered.reshape(LEN, head_count, head_size)

def reference(hidden_in, sb_query_w, sb_key_w, sb_value_w, sb_offset, delta_query_w, delta_key_w, delta_value_w, decay_w, write_w, write_bias, decay_log_scale, decay_shift, head_gain, sb_out_w, delta_out_w):

    def one_sequence(inputs):
        sequence_rows, shift_rows = inputs

        def project(weight):
            return jnp.dot(sequence_rows, weight, preferred_element_type=jnp.float32).astype(jnp.bfloat16)
        sb_query = project(sb_query_w).reshape(LEN, SB_HEADS, SB_DIM)
        sb_keys = project(sb_key_w).reshape(LEN, SB_HEADS, SB_DIM)
        sb_values = project(sb_value_w).reshape(LEN, SB_HEADS, SB_DIM)
        sb_mixed = stick_sequence(sb_query, sb_keys, sb_values, sb_offset).astype(jnp.bfloat16).reshape(LEN, SB_HEADS * SB_DIM)
        decay_pre = jnp.dot(sequence_rows, decay_w, preferred_element_type=jnp.float32)
        write_pre = jnp.dot(sequence_rows, write_w, preferred_element_type=jnp.float32)
        queries, key_rows, value_rows, log_decay, strength = delta_inputs(project(delta_query_w), project(delta_key_w), project(delta_value_w), decay_pre, write_pre, write_bias, decay_log_scale, shift_rows.T, GDN_HEADS, GDN_DIM)
        prepared = delta_prepare(to_blocks(queries, BLOCK), to_blocks(key_rows, BLOCK), to_blocks(value_rows, BLOCK), to_blocks(log_decay, BLOCK), to_blocks(strength, BLOCK))
        initial = jnp.zeros((GDN_HEADS, GDN_DIM, GDN_DIM), jnp.float32)
        unused_memory, produced_rows = lax.scan(delta_step, initial, prepared)
        produced_rows = from_blocks(produced_rows)
        normed = produced_rows * lax.rsqrt(lax.optimization_barrier(jnp.mean(produced_rows * produced_rows, axis=-1, keepdims=True)) + NORM_EPS) * head_gain
        delta_mixed = normed.astype(jnp.bfloat16).reshape(LEN, GDN_HEADS * GDN_DIM)
        sb_group = SB_HEADS * SB_DIM // N_TP
        delta_group = GDN_HEADS * GDN_DIM // N_TP
        accumulated = jnp.zeros((LEN, D), jnp.float32)
        for group_number in range(N_TP):
            sb_cols = slice(group_number * sb_group, (group_number + 1) * sb_group)
            delta_cols = slice(group_number * delta_group, (group_number + 1) * delta_group)
            term = jnp.dot(sb_mixed[:, sb_cols], sb_out_w[sb_cols], preferred_element_type=jnp.float32) + jnp.dot(delta_mixed[:, delta_cols], delta_out_w[delta_cols], preferred_element_type=jnp.float32)
            rounded = lax.optimization_barrier(term.astype(jnp.bfloat16))
            accumulated = accumulated + rounded.astype(jnp.float32)
        return accumulated.astype(jnp.bfloat16)
    return lax.map(one_sequence, (hidden_in, decay_shift))
```

```python
import functools

import jax
import jax.numpy as jnp
import numpy as np
from jax import lax
from jax.experimental import pallas as pl
from jax.experimental.pallas import tpu as pltpu
from jax.sharding import Mesh
from jax.sharding import PartitionSpec as P

f32 = jnp.float32
bf16 = jnp.bfloat16
LOG2E = float(np.log2(np.e))
EPS = 1e-6
CH = 256
NT = (((1,), (1,)), ((), ()))
Z = ("zh", "zl")
AXES = ("zh", "zl", "y", "fs", "tp")


def work_lists():
    place = lambda i, m, y: (m % 4) * 8 + (4 * i + y - m) // 4
    pairs = np.zeros((4, 2, 64), np.int32)
    single = np.zeros((4, 4, 8), np.int32)
    for y in range(4):
        steps = [(p, place(2 * p, m, y)) for p in (3, 2, 1, 0) for m in range(1, 8 * p + y + 1)]
        pairs[y, :, : len(steps)] = np.array(steps).T
        for chain, ps in enumerate(((3, 1), (2, 0))):
            steps = [(2 * p + 1, place(2 * p + 1, m, y)) for p in ps for m in range(1, 5)]
            single[y, 2 * chain : 2 * chain + 2] = np.array(steps).T
    return pairs, single


def stick_kernel(count_ref, pairs_ref, single_ref, off_ref, q_ref, kv_ref, u_ref, o_ref, acc, run, kt):
    off = off_ref[0]

    def turn(c, carry):
        kt[c] = jnp.transpose(kv_ref[c])
        return carry

    lax.fori_loop(0, 32, turn, 0, unroll=4)

    def tile(first_row, size, c, masked):
        rows = pl.ds(first_row, size)
        kv = kv_ref[c]
        z = jnp.dot(q_ref[rows, :], kt[c], preferred_element_type=f32) * (0.125 * LOG2E) + off
        sp = jnp.maximum(jnp.log2(1.0 + jnp.exp2(jnp.minimum(z, 40.0))), z)
        if masked:
            shape = (size, CH)
            seen = lax.broadcasted_iota(jnp.int32, shape, 1) < lax.broadcasted_iota(jnp.int32, shape, 0)
            sp = jnp.where(seen, sp, 0.0)
        after = jnp.dot(sp.astype(bf16), u_ref[...], preferred_element_type=f32)
        total = after[:, :1] + sp[:, :1]
        if masked:
            w = jnp.where(seen, jnp.exp2((z - sp) - after), 0.0)
            run[rows, :] = jnp.broadcast_to(total, (size, 128))
            acc[rows, :] = jnp.dot(w.astype(bf16), kv, preferred_element_type=f32)
        else:
            r = run[rows, :]
            w = jnp.exp2((z - sp) - (after + jnp.concatenate([r, r], axis=1)))
            run[rows, :] = r + total
            acc[rows, :] += jnp.dot(w.astype(bf16), kv, preferred_element_type=f32)

    def diagonal(n, carry):
        for k in range(2):
            tile(pl.multiple_of((2 * n + k) * CH, CH), CH, 2 * n + k, True)
        return carry

    lax.fori_loop(0, 4, diagonal, 0)

    def one(n, carry):
        for k in range(2):
            tile(pl.multiple_of(single_ref[2 * k, n] * CH, CH), CH, single_ref[2 * k + 1, n], False)
        return carry

    lax.fori_loop(0, 8, one, 0)

    def both(n, carry):
        tile(pl.multiple_of(pairs_ref[0, n] * 2 * CH, 2 * CH), 2 * CH, pairs_ref[1, n], False)
        return carry

    lax.fori_loop(0, count_ref[0], both, 0)
    lane = lax.broadcasted_iota(jnp.int32, (64, 128), 1)
    for d in range(16):
        low = acc[d * 128 : d * 128 + 64, :]
        high = acc[d * 128 + 64 : d * 128 + 128, :]
        o_ref[d] = jnp.where(lane < 64, pltpu.roll(low, 64, 1), high).astype(bf16)


def stick_attention(count, pairs, single, off, q, kv, u):
    smem = pl.BlockSpec(memory_space=pltpu.SMEM)
    vmem = pl.BlockSpec(memory_space=pltpu.VMEM)
    return pl.pallas_call(
        stick_kernel,
        out_shape=jax.ShapeDtypeStruct((16, 64, 128), bf16),
        in_specs=[smem] * 4 + [vmem] * 3,
        out_specs=vmem,
        scratch_shapes=[
            pltpu.VMEM((2048, 128), f32),
            pltpu.VMEM((2048, 128), f32),
            pltpu.VMEM((32, 128, CH), bf16),
        ],
        cost_estimate=pl.CostEstimate(flops=20_000_000_000, bytes_accessed=4_000_000, transcendentals=26_000_000),
        name="stick_attention",
    )(count, pairs, single, off, q, kv, u)


def mm(a, b, dims=(((1,), (0,)), ((), ()))):
    return lax.dot_general(a.astype(bf16), b.astype(bf16), dims, preferred_element_type=f32)


def silu(u):
    return u * jax.nn.sigmoid(u)


def unit(u):
    return u * lax.rsqrt(jnp.sum(u * u, axis=-1, keepdims=True) + EPS)


def delta_kernel(par_ref, proj_ref, shift_ref, qf_ref, of_ref, end_ref):
    minus_scale, bias = par_ref[0], par_ref[1]
    span = (CH, CH)
    row = lax.broadcasted_iota(jnp.int32, span, 0)
    col = lax.broadcasted_iota(jnp.int32, span, 1)
    same = (row // 64) == (col // 64)
    inclusive = jnp.logical_and(same, col <= row)
    strict = jnp.logical_and(same, col < row)
    sums = jnp.concatenate([jnp.where(inclusive, 1.0, 0.0), jnp.where(same, 1.0, 0.0)], axis=0)
    eye = jnp.where(row == col, 1.0, 0.0)
    lane = lax.broadcasted_iota(jnp.int32, (CH, 128), 1)
    tiles = range(4)
    cum, tot, q, k, v, beta = [], [], [], [], [], []
    for t in tiles:
        rows = slice(t * CH, (t + 1) * CH)
        proj = proj_ref[rows, :]
        dq, dk, dv = (proj[:, 128 * n : 128 * n + 128].astype(bf16).astype(f32) for n in range(3))
        pre = proj[:, 384:385]
        softplus = jnp.maximum(pre, 0.0) + jnp.log1p(jnp.exp(-jnp.abs(pre)))
        g = minus_scale * softplus + shift_ref[rows, :]
        beta.append(jax.nn.sigmoid(proj[:, 385:386] + bias))
        q.append(unit(silu(dq)) * 128**-0.5)
        k.append(unit(silu(dk)))
        v.append(silu(dv))
        g1 = g.astype(bf16).astype(f32)
        g2 = (g - g1).astype(bf16).astype(f32)
        g3 = g - g1 - g2
        parts = jnp.where(lane == 0, g1, jnp.where(lane == 1, g2, jnp.where(lane == 2, g3, 0.0)))
        s = mm(sums, parts)
        s = jnp.broadcast_to(s[:, 0:1] + s[:, 1:2] + s[:, 2:3], (2 * CH, 128))
        cum.append(s[:CH])
        tot.append(s[CH:])
    table = []
    for t in tiles:
        across = jnp.transpose(cum[t])[0:1, :]
        spread = cum[t][:, 0:1] - across
        table.append(jnp.where(inclusive, jnp.exp(jnp.where(inclusive, spread, 0.0)), 0.0))
    keys_beta = [k[t] * beta[t] for t in tiles]
    power = [jnp.where(strict, mm(keys_beta[t], k[t], NT) * table[t], 0.0) for t in tiles]
    inside = [mm(q[t], k[t], NT) * table[t] for t in tiles]
    inverse = [eye - power[t] for t in tiles]
    for _ in range(5):
        power = [mm(power[t], power[t]) for t in tiles]
        inverse = [inverse[t] + mm(inverse[t], power[t]) for t in tiles]
    growth = [jnp.exp(cum[t]) for t in tiles]
    both = [
        mm(inverse[t], jnp.concatenate([keys_beta[t] * growth[t], v[t] * beta[t]], axis=1)) for t in tiles
    ]
    seen = [mm(inside[t], both[t]) for t in tiles]
    reach = [q[t] * growth[t] - seen[t][:, :128] for t in tiles]
    own = [seen[t][:, 128:] for t in tiles]
    damped = [jnp.transpose(k[t] * jnp.exp(tot[t] - cum[t])) for t in tiles]
    wide = lax.broadcasted_iota(jnp.int32, (128, CH), 1) // 64
    small_eye = jnp.where(
        lax.broadcasted_iota(jnp.int32, (128, 128), 0) == lax.broadcasted_iota(jnp.int32, (128, 128), 1), 1.0, 0.0
    )
    maps = []
    for t in tiles:
        masked = jnp.concatenate([jnp.where(wide == b, damped[t], 0.0) for b in range(4)], axis=0)
        moved = mm(masked, both[t])
        for b in range(4):
            decay = jnp.exp(tot[t][b * 64 : b * 64 + 1, :])
            piece = moved[b * 128 : b * 128 + 128]
            maps.append((small_eye * decay - piece[:, :128], piece[:, 128:]))
    state = jnp.concatenate([small_eye, jnp.zeros((128, 128), f32)], axis=1)
    for n in range(16):
        t, b = n // 4, n % 4
        rows = slice(n * 64, n * 64 + 64)
        out = mm(reach[t][b * 64 : b * 64 + 64], state)
        qf_ref[rows, :] = out[:, :128]
        of_ref[rows, :] = out[:, 128:] + own[t][b * 64 : b * 64 + 64]
        state = mm(maps[n][0], state)
        state = jnp.concatenate([state[:, :128], state[:, 128:] + maps[n][1]], axis=1)
    end_ref[...] = state.astype(bf16)


def delta_local(par, proj, shift):
    vmem = pl.BlockSpec(memory_space=pltpu.VMEM)
    return pl.pallas_call(
        delta_kernel,
        out_shape=(
            jax.ShapeDtypeStruct((1024, 128), f32),
            jax.ShapeDtypeStruct((1024, 128), f32),
            jax.ShapeDtypeStruct((128, 256), bf16),
        ),
        in_specs=[pl.BlockSpec(memory_space=pltpu.SMEM), vmem, vmem],
        out_specs=(vmem, vmem, vmem),
        cost_estimate=pl.CostEstimate(flops=8_000_000_000, bytes_accessed=4_000_000, transcendentals=1_000_000),
        name="delta_local",
    )(par, proj, shift)


def finish_kernel(gain_ref, qf_ref, of_ref, *refs):
    maps, o_ref = refs[:-1], refs[-1]
    state = jnp.zeros((128, 128), f32)
    for ref in maps:
        state = mm(ref[:, :128], state) + ref[:, 128:].astype(f32)
    for t in range(4):
        rows = slice(t * CH, (t + 1) * CH)
        o = mm(qf_ref[rows, :], state) + of_ref[rows, :]
        o = o * lax.rsqrt(jnp.mean(o * o, axis=-1, keepdims=True) + EPS) * gain_ref[...]
        o_ref[rows, :] = o.astype(bf16)


def delta_finish(gain, qf, of, maps):
    vmem = pl.BlockSpec(memory_space=pltpu.VMEM)
    return pl.pallas_call(
        finish_kernel,
        out_shape=jax.ShapeDtypeStruct((1024, 128), bf16),
        in_specs=[vmem] * (3 + len(maps)),
        out_specs=vmem,
        cost_estimate=pl.CostEstimate(flops=1_000_000_000, bytes_accessed=2_000_000, transcendentals=2_000),
        name="delta_finish",
    )(gain, qf, of, *maps)


def ring(axis, size, step):
    return functools.partial(lax.ppermute, axis_name=axis, perm=[(i, (i + step) % size) for i in range(size)])


def placed(pieces, index, size, rows):
    whole = jnp.zeros((size * rows, *pieces[0].shape[1:]), pieces[0].dtype)
    for d, piece in enumerate(pieces):
        whole = lax.dynamic_update_slice_in_dim(whole, piece, ((index - d) % size) * rows, 0)
    return whole


def on_device(
    hidden_in,
    sb_query_w,
    sb_key_w,
    sb_value_w,
    sb_offset,
    delta_query_w,
    delta_key_w,
    delta_value_w,
    decay_w,
    write_w,
    write_bias,
    decay_log_scale,
    decay_shift,
    head_gain,
    sb_out_w,
    delta_out_w,
):
    z, y, fs, tp = lax.axis_index(Z), lax.axis_index("y"), lax.axis_index("fs"), lax.axis_index("tp")
    x = hidden_in.reshape(256, 1024)
    x_z = lax.all_gather(x, ("tp", *Z), axis=0, tiled=False).reshape(2, 2048, 1024)

    pick = lambda w, at, n: lax.dynamic_slice_in_dim(w, at, n, 1)
    mine = jnp.concatenate(
        [pick(sb_query_w, z * 64, 64), jnp.zeros((512, 64), bf16), pick(sb_key_w, z * 64, 64), pick(sb_value_w, z * 64, 64)]
        + [pick(w, y * 128, 128) for w in (delta_query_w, delta_key_w, delta_value_w)],
        axis=1,
    )
    weights = [mine] + [ring("fs", 4, d)(mine) for d in (1, 2, 3)]

    x_own = placed([x] + [ring("y", 4, d)(x) for d in (1, 2, 3)], y, 4, 256)
    swap = functools.partial(lax.ppermute, axis_name="tp", perm=[(0, 1), (1, 0)])
    x_other = swap(x_own)
    shift = decay_shift.reshape(4, 256)
    shifts = [shift] + [ring("y", 4, d)(shift) for d in (1, 2, 3)]
    shift_col = placed([pick(s.T, y, 1) for s in shifts], y, 4, 256)
    out_w = jnp.concatenate([sb_out_w, delta_out_w], axis=0)
    out_other = swap(out_w)

    w_all = placed(weights, fs, 4, 512)
    side = jnp.concatenate([pick(decay_w, y, 1), pick(write_w, y, 1), jnp.zeros((2048, 126), bf16)], axis=1)
    w_delta = jnp.concatenate([w_all[:, 256:], side], axis=1).reshape(2, 1024, 512)
    half = lambda w, at: lax.dynamic_index_in_dim(w, at, 0, keepdims=False)
    proj = jnp.dot(x_own, half(w_delta, tp), preferred_element_type=f32) + jnp.dot(
        x_other, half(w_delta, 1 - tp), preferred_element_type=f32
    )
    par = jnp.stack(
        [
            -jnp.exp(lax.dynamic_index_in_dim(decay_log_scale, y, 0, keepdims=False)),
            lax.dynamic_index_in_dim(write_bias, y, 0, keepdims=False),
        ]
    )
    qf, of, end = delta_local(par, proj, shift_col)
    ends = [lax.ppermute(end, Z, [(i, i + d) for i in range(8 - d)]) for d in range(7, 0, -1)]

    w_stick = w_all[:, :256]
    stick = (
        jnp.dot(x_z[0], w_stick[:1024], preferred_element_type=f32)
        + jnp.dot(x_z[1], w_stick[1024:], preferred_element_type=f32)
    ).astype(bf16)
    q, kv = stick[:, :128], stick[:, 128:]
    kv_all = jnp.concatenate([kv] + [ring("y", 4, d)(kv) for d in (1, 2, 3)], axis=0).reshape(32, CH, 128)
    pairs, single = work_lists()
    at_y = lambda table: lax.dynamic_index_in_dim(jnp.asarray(table), y, 0, keepdims=False)
    u = jnp.asarray(np.tril(np.ones((CH, CH), np.float32), -1), bf16)
    offset = lax.dynamic_slice_in_dim(sb_offset, z, 1, 0) * LOG2E
    count = (48 + 4 * y).astype(jnp.int32).reshape(1)
    sb = stick_attention(count, at_y(pairs), at_y(single), offset, q, kv_all, u)
    sb = lax.all_to_all(sb, (*Z, "tp"), 0, 0, tiled=True)

    dm = delta_finish(head_gain.reshape(1, 128), qf, of, ends)
    dm = lax.all_to_all(dm.reshape(8, 128, 128), ("y", "tp"), 0, 0, tiled=True)

    sb = sb.reshape(8, 2, 64, 2, 64).transpose(1, 3, 2, 0, 4).reshape(2, 128, 512)
    dm = dm.reshape(4, 2, 128, 128).transpose(1, 2, 0, 3).reshape(2, 128, 512)
    mixed = jnp.concatenate([sb, dm], axis=2)
    out = jnp.dot(half(mixed, tp), out_w, preferred_element_type=f32) + jnp.dot(
        half(mixed, 1 - tp), out_other, preferred_element_type=f32
    )
    return out.astype(bf16).reshape(1, 128, 2048)


def solution(mesh):
    finer = Mesh(mesh.devices.reshape(2, 4, 4, mesh.shape["fs"], mesh.shape["tp"]), AXES)
    sp = ("zh", "zl", "y")
    return jax.shard_map(
        on_device,
        mesh=finer,
        in_specs=(
            P("fs", sp, "tp"),
            P("fs", "tp"),
            P("fs", "tp"),
            P("fs", "tp"),
            P("tp"),
            P("fs", "tp"),
            P("fs", "tp"),
            P("fs", "tp"),
            P(None, "tp"),
            P(None, "tp"),
            P("tp"),
            P("tp"),
            P("fs", "tp", sp),
            P(),
            P("tp", None),
            P("tp", None),
        ),
        out_specs=P("fs", (*sp, "tp"), None),
        check_vma=False,
    )
```

```python
import functools

import jax
import jax.numpy as jnp
import numpy as np
from jax import lax
from jax.experimental import pallas as pl
from jax.experimental.pallas import tpu as pltpu
from jax.sharding import Mesh
from jax.sharding import PartitionSpec as P


f32 = jnp.float32
bf16 = jnp.bfloat16
LOG2E = float(np.log2(np.e))
EPS = 1e-6
CH = 256
NT = (((1,), (1,)), ((), ()))
Z = ("zh", "zl")
AXES = ("zh", "zl", "y", "fs", "tp")


SLOT = (0, 2, 4, 6, 7, 5, 3, 1)
PAIRS, SINGLE, SLOTS, COUNT, HEAD = 0, 256, 320, 328, 329


def work_list():
    table = np.zeros((32, 384), np.int32)
    for z in range(8):
        slot = lambda i: SLOT[(i - z) % 8]
        for y in range(4):
            row = table[4 * z + y]
            place = lambda i, m: (m % 4) * 8 + slot((4 * i + y - m) // 4)
            steps = [(slot(2 * p), slot(2 * p + 1), place(2 * p, m)) for p in (3, 2, 1, 0) for m in range(1, 8 * p + y + 1)]
            for n, step in enumerate(steps):
                for k in range(3):
                    row[PAIRS + 64 * k + n] = step[k]
            for chain, ps in enumerate(((3, 1), (2, 0))):
                steps_one = [(slot(2 * p + 1), place(2 * p + 1, m)) for p in ps for m in range(1, 5)]
                for n, step in enumerate(steps_one):
                    row[SINGLE + 16 * chain + n] = step[0]
                    row[SINGLE + 16 * chain + 8 + n] = step[1]
            row[SLOTS : SLOTS + 8] = [slot(i) for i in range(8)]
            row[COUNT], row[HEAD] = len(steps), z
    return table


def stick_kernel(table, off_ref, qa_ref, qb_ref, u_ref, *refs):
    kv_refs, o_ref, (acc, run, q, kvs, kt) = refs[:8], refs[8], refs[9:]
    off = off_ref[table[HEAD]] * LOG2E
    for n in range(5):
        q[n] = qa_ref[n]
    for n in range(3):
        q[5 + n] = qb_ref[n]
    for d in range(4):
        for n in range(8):
            block = kv_refs[d][n] if n < 5 else kv_refs[4 + d][n - 5]
            kvs[d * 8 + n] = block
            kt[d * 8 + n] = jnp.transpose(block)

    def tile(slots, c, masked):
        size = CH * len(slots)
        join = lambda ref: jnp.concatenate([ref[s] for s in slots], axis=0) if len(slots) > 1 else ref[slots[0]]
        kv = kvs[c]
        z = jnp.dot(join(q), kt[c], preferred_element_type=f32) * (0.125 * LOG2E) + off
        sp = jnp.maximum(jnp.log2(1.0 + jnp.exp2(jnp.minimum(z, 40.0))), z)
        if masked:
            shape = (size, CH)
            seen = lax.broadcasted_iota(jnp.int32, shape, 1) < lax.broadcasted_iota(jnp.int32, shape, 0)
            sp = jnp.where(seen, sp, 0.0)
        after = jnp.dot(sp.astype(bf16), u_ref[...], preferred_element_type=f32)
        total = after[:, :1] + sp[:, :1]
        if masked:
            w = jnp.where(seen, jnp.exp2((z - sp) - after), 0.0)
            total = jnp.broadcast_to(total, (size, 128))
            out = jnp.dot(w.astype(bf16), kv, preferred_element_type=f32)
        else:
            r = join(run)
            w = jnp.exp2((z - sp) - (after + jnp.concatenate([r, r], axis=1)))
            total = r + total
            out = join(acc) + jnp.dot(w.astype(bf16), kv, preferred_element_type=f32)
        for k, s in enumerate(slots):
            run[s] = total[k * CH : k * CH + CH]
            acc[s] = out[k * CH : k * CH + CH]

    def diagonal(n, carry):
        for k in range(2):
            tile((2 * n + k,), 2 * n + k, True)
        return carry

    lax.fori_loop(0, 4, diagonal, 0)

    def one(n, carry):
        for k in range(2):
            tile((table[SINGLE + 16 * k + n],), table[SINGLE + 16 * k + 8 + n], False)
        return carry

    lax.fori_loop(0, 8, one, 0)

    def both(n, carry):
        tile((table[PAIRS + n], table[PAIRS + 64 + n]), table[PAIRS + 128 + n], False)
        return carry

    lax.fori_loop(0, table[COUNT], both, 0)
    lane = lax.broadcasted_iota(jnp.int32, (64, 128), 1)
    for i in range(8):
        rows = acc[table[SLOTS + i]]
        for h in range(2):
            low, high = rows[128 * h : 128 * h + 64], rows[128 * h + 64 : 128 * h + 128]
            o_ref[2 * i + h] = jnp.where(lane < 64, pltpu.roll(low, 64, 1), high).astype(bf16)


def stick_attention(table, off, qa, qb, u, kvs):
    smem = pl.BlockSpec(memory_space=pltpu.SMEM)
    vmem = pl.BlockSpec(memory_space=pltpu.VMEM)
    return pl.pallas_call(
        stick_kernel,
        out_shape=jax.ShapeDtypeStruct((16, 64, 128), bf16),
        in_specs=[smem] * 2 + [vmem] * (3 + len(kvs)),
        out_specs=vmem,
        scratch_shapes=[
            pltpu.VMEM((8, CH, 128), f32),
            pltpu.VMEM((8, CH, 128), f32),
            pltpu.VMEM((8, CH, 128), bf16),
            pltpu.VMEM((32, CH, 128), bf16),
            pltpu.VMEM((32, 128, CH), bf16),
        ],
        cost_estimate=pl.CostEstimate(flops=20_000_000_000, bytes_accessed=4_000_000, transcendentals=26_000_000),
        name="stick_attention",
    )(table, off, qa, qb, u, *kvs)


def project_rows(w_ref, own, other, q_ref, kv_ref):
    at = 0
    for a, b in zip(own, other):
        rows = a.shape[0]
        out = jnp.dot(a[...], w_ref[:1024], preferred_element_type=f32)
        out = (out + jnp.dot(b[...], w_ref[1024:], preferred_element_type=f32)).astype(bf16)
        n, first = at // CH, at % CH
        q_ref[n, first : first + rows, :] = out[:, :128]
        kv_ref[n, first : first + rows, :] = out[:, 128:]
        at += rows


def first_project_kernel(place, *refs):
    weights, x, (q_ref, kv_ref, w_ref, w_all) = refs[:4], refs[4:-4], refs[-4:]
    fs, tp = place[1], place[2]
    for d in range(4):
        w_all[lax.rem(fs - d + 4, 4)] = weights[d][:, :256]
    for h in range(2):
        for j in range(2):
            w_ref[h * 1024 + j * 512 : h * 1024 + j * 512 + 512, :] = w_all[2 * (tp if h == 0 else 1 - tp) + j]
    project_rows(w_ref, x[: len(x) // 2], x[len(x) // 2 :], q_ref, kv_ref)


def later_project_kernel(w_ref, *refs):
    x, (q_ref, kv_ref) = refs[:-2], refs[-2:]
    project_rows(w_ref, x[: len(x) // 2], x[len(x) // 2 :], q_ref, kv_ref)


def stick_project(place, weights, own, other):
    vmem = pl.BlockSpec(memory_space=pltpu.VMEM)
    n = sum(a.shape[0] for a in own) // CH
    shape = jax.ShapeDtypeStruct((n, CH, 128), bf16)
    cost = pl.CostEstimate(flops=n * 270_000_000, bytes_accessed=n * 1_200_000, transcendentals=0)
    if place is None:
        return pl.pallas_call(
            later_project_kernel,
            out_shape=(shape, shape),
            in_specs=[vmem] * (1 + len(own) + len(other)),
            out_specs=(vmem, vmem),
            cost_estimate=cost,
            name="stick_project_b",
        )(weights, *own, *other)
    return pl.pallas_call(
        first_project_kernel,
        out_shape=(shape, shape, jax.ShapeDtypeStruct((2048, 256), bf16)),
        in_specs=[pl.BlockSpec(memory_space=pltpu.SMEM)] + [vmem] * (4 + len(own) + len(other)),
        out_specs=(vmem, vmem, vmem),
        scratch_shapes=[pltpu.VMEM((4, 512, 256), bf16)],
        cost_estimate=cost,
        name="stick_project_a",
    )(place, *weights, *own, *other)


def mm(a, b, dims=(((1,), (0,)), ((), ()))):
    return lax.dot_general(a.astype(bf16), b.astype(bf16), dims, preferred_element_type=f32)


def silu(u):
    return u * jax.nn.sigmoid(u)


def unit(u):
    return u * lax.rsqrt(jnp.sum(u * u, axis=-1, keepdims=True) + EPS)


def delta_kernel(place, scale_ref, bias_ref, decay_ref, write_ref, *refs):
    weights, own, other, shifts = refs[:4], refs[4:8], refs[8:12], refs[12:16]
    qf_ref, of_ref, end_ref, w_all, proj_all = refs[16:]
    y, fs, tp = place[0], place[1], place[2]
    minus_scale = -jnp.exp(jnp.full((CH, 1), scale_ref[y], f32))
    bias = bias_ref[y]
    for d in range(4):
        w_all[lax.rem(fs - d + 4, 4)] = weights[d][:, 256:]
    narrow = lax.broadcasted_iota(jnp.int32, (CH, 4), 1)
    for d in range(4):
        out, pre = 0.0, [0.0, 0.0]
        for h, x in ((0, own[d]), (1, other[d])):
            mine = tp if h == 0 else 1 - tp
            for j in range(2):
                part = x[:, j * 512 : j * 512 + 512]
                block = 2 * mine + j
                out += jnp.dot(part, w_all[block], preferred_element_type=f32)
                columns = pl.ds(pl.multiple_of(block * 512, 512), 512)
                pre[0] += lax.dot_general(part, decay_ref[:, columns], NT, preferred_element_type=f32)
                pre[1] += lax.dot_general(part, write_ref[:, columns], NT, preferred_element_type=f32)
        pre = [jnp.sum(jnp.where(narrow == y, p, 0.0), axis=1, keepdims=True) for p in pre]
        lanes = lax.broadcasted_iota(jnp.int32, (CH, 128), 1)
        shift = jnp.transpose(jnp.broadcast_to(shifts[d][pl.ds(y, 1), :], (128, CH)))
        side = jnp.where(lanes == 0, pre[0], jnp.where(lanes == 1, pre[1], shift))
        proj_all[lax.rem(y - d + 4, 4)] = jnp.concatenate([out, side], axis=1)
    span = (CH, CH)
    row = lax.broadcasted_iota(jnp.int32, span, 0)
    col = lax.broadcasted_iota(jnp.int32, span, 1)
    same = (row // 64) == (col // 64)
    inclusive = jnp.logical_and(same, col <= row)
    strict = jnp.logical_and(same, col < row)
    sums = jnp.concatenate([jnp.where(inclusive, 1.0, 0.0), jnp.where(same, 1.0, 0.0)], axis=0)
    eye = jnp.where(row == col, 1.0, 0.0)
    lane = lax.broadcasted_iota(jnp.int32, (CH, 128), 1)
    tiles = range(4)
    cum, tot, q, k, v, beta = [], [], [], [], [], []
    for t in tiles:
        proj = proj_all[t]
        dq, dk, dv = (proj[:, 128 * n : 128 * n + 128].astype(bf16).astype(f32) for n in range(3))
        pre = proj[:, 384:385]
        softplus = jnp.maximum(pre, 0.0) + jnp.log1p(jnp.exp(-jnp.abs(pre)))
        g = minus_scale * softplus + proj[:, 386:387]
        beta.append(jax.nn.sigmoid(proj[:, 385:386] + bias))
        q.append(unit(silu(dq)) * 128**-0.5)
        k.append(unit(silu(dk)))
        v.append(silu(dv))
        g1 = g.astype(bf16).astype(f32)
        g2 = (g - g1).astype(bf16).astype(f32)
        g3 = g - g1 - g2
        parts = jnp.where(lane == 0, g1, jnp.where(lane == 1, g2, jnp.where(lane == 2, g3, 0.0)))
        s = mm(sums, parts)
        s = jnp.broadcast_to(s[:, 0:1] + s[:, 1:2] + s[:, 2:3], (2 * CH, 128))
        cum.append(s[:CH])
        tot.append(s[CH:])
    table = []
    for t in tiles:
        across = jnp.transpose(cum[t])[0:1, :]
        spread = cum[t][:, 0:1] - across
        table.append(jnp.where(inclusive, jnp.exp(jnp.where(inclusive, spread, 0.0)), 0.0))
    keys_beta = [k[t] * beta[t] for t in tiles]
    power = [jnp.where(strict, mm(keys_beta[t], k[t], NT) * table[t], 0.0) for t in tiles]
    inside = [mm(q[t], k[t], NT) * table[t] for t in tiles]
    inverse = [eye - power[t] for t in tiles]
    for _ in range(5):
        power = [mm(power[t], power[t]) for t in tiles]
        inverse = [inverse[t] + mm(inverse[t], power[t]) for t in tiles]
    growth = [jnp.exp(cum[t]) for t in tiles]
    both = [
        mm(inverse[t], jnp.concatenate([keys_beta[t] * growth[t], v[t] * beta[t]], axis=1)) for t in tiles
    ]
    seen = [mm(inside[t], both[t]) for t in tiles]
    reach = [q[t] * growth[t] - seen[t][:, :128] for t in tiles]
    own = [seen[t][:, 128:] for t in tiles]
    damped = [jnp.transpose(k[t] * jnp.exp(tot[t] - cum[t])) for t in tiles]
    wide = lax.broadcasted_iota(jnp.int32, (128, CH), 1) // 64
    small_eye = jnp.where(
        lax.broadcasted_iota(jnp.int32, (128, 128), 0) == lax.broadcasted_iota(jnp.int32, (128, 128), 1), 1.0, 0.0
    )
    maps = []
    for t in tiles:
        masked = jnp.concatenate([jnp.where(wide == b, damped[t], 0.0) for b in range(4)], axis=0)
        moved = mm(masked, both[t])
        for b in range(4):
            decay = jnp.exp(tot[t][b * 64 : b * 64 + 1, :])
            piece = moved[b * 128 : b * 128 + 128]
            maps.append((small_eye * decay - piece[:, :128], piece[:, 128:]))
    state = jnp.concatenate([small_eye, jnp.zeros((128, 128), f32)], axis=1)
    for n in range(16):
        t, b = n // 4, n % 4
        rows = slice(n * 64, n * 64 + 64)
        out = mm(reach[t][b * 64 : b * 64 + 64], state)
        qf_ref[rows, :] = out[:, :128]
        of_ref[rows, :] = out[:, 128:] + own[t][b * 64 : b * 64 + 64]
        state = mm(maps[n][0], state)
        state = jnp.concatenate([state[:, :128], state[:, 128:] + maps[n][1]], axis=1)
    end_ref[...] = state.astype(bf16)


def delta_local(place, scale, bias, decay_w, write_w, weights, own, other, shifts):
    smem = pl.BlockSpec(memory_space=pltpu.SMEM)
    vmem = pl.BlockSpec(memory_space=pltpu.VMEM)
    return pl.pallas_call(
        delta_kernel,
        out_shape=(
            jax.ShapeDtypeStruct((1024, 128), f32),
            jax.ShapeDtypeStruct((1024, 128), f32),
            jax.ShapeDtypeStruct((128, 256), bf16),
        ),
        in_specs=[smem] * 3 + [vmem] * 18,
        out_specs=(vmem,) * 3,
        scratch_shapes=[pltpu.VMEM((4, 512, 384), bf16), pltpu.VMEM((4, CH, 512), f32)],
        cost_estimate=pl.CostEstimate(flops=12_000_000_000, bytes_accessed=8_000_000, transcendentals=1_000_000),
        name="delta_local",
    )(place, scale, bias, decay_w, write_w, *weights, *own, *other, *shifts)


def finish_kernel(gain_ref, qf_ref, of_ref, *refs):
    maps, o_ref = refs[:-1], refs[-1]
    state = jnp.zeros((128, 128), f32)
    for ref in maps:
        state = mm(ref[:, :128], state) + ref[:, 128:].astype(f32)
    for t in range(4):
        rows = slice(t * CH, (t + 1) * CH)
        o = mm(qf_ref[rows, :], state) + of_ref[rows, :]
        o = o * lax.rsqrt(jnp.mean(o * o, axis=-1, keepdims=True) + EPS) * gain_ref[...]
        o_ref[rows, :] = o.astype(bf16)


def delta_finish(gain, qf, of, maps):
    vmem = pl.BlockSpec(memory_space=pltpu.VMEM)
    return pl.pallas_call(
        finish_kernel,
        out_shape=jax.ShapeDtypeStruct((1024, 128), bf16),
        in_specs=[vmem] * (3 + len(maps)),
        out_specs=vmem,
        cost_estimate=pl.CostEstimate(flops=1_000_000_000, bytes_accessed=2_000_000, transcendentals=2_000),
        name="delta_finish",
    )(gain, qf, of, *maps)


def ring(axis, size, step):
    return functools.partial(lax.ppermute, axis_name=axis, perm=[(i, (i + step) % size) for i in range(size)])


def on_device(
    hidden_in,
    sb_query_w,
    sb_key_w,
    sb_value_w,
    sb_offset,
    delta_query_w,
    delta_key_w,
    delta_value_w,
    decay_w,
    write_w,
    write_bias,
    decay_log_scale,
    decay_shift,
    head_gain,
    sb_out_w,
    delta_out_w,
):
    z, y, fs, tp = lax.axis_index(Z), lax.axis_index("y"), lax.axis_index("fs"), lax.axis_index("tp")
    x = hidden_in.reshape(256, 1024)

    across = functools.partial(lax.ppermute, axis_name="tp", perm=[(0, 1), (1, 0)])
    swap = lambda v: across(v)
    right, left = ring(Z, 8, 1), ring(Z, 8, 7)
    around = lambda axis, v: [v] + [ring(axis, 4, d)(v) for d in (1, 2, 3)]
    pick = lambda w, at, n: lax.dynamic_slice_in_dim(w, at, n, 1)
    item = lambda v, at: lax.dynamic_index_in_dim(v, at, 0, keepdims=False)

    mine = jnp.concatenate(
        [pick(sb_query_w, z * 64, 64), jnp.zeros((512, 64), bf16), pick(sb_key_w, z * 64, 64), pick(sb_value_w, z * 64, 64)]
        + [pick(w, y * 128, 128) for w in (delta_query_w, delta_key_w, delta_value_w)],
        axis=1,
    )
    r1, l1 = right(x), left(x)
    at_y = around("y", x)
    weights = around("fs", mine)
    r2, l2 = right(r1), left(l1)
    r3, l3 = right(r2), left(l2)
    r4, l4 = right(r3[:128]), left(l3[128:])
    other_y = [swap(v) for v in at_y]
    other_r = [swap(v) for v in (r1, r2, r3, r4)]
    other_l = [swap(v) for v in (l1, l2, l3, l4)]
    shifts = around("y", decay_shift.reshape(4, 256))

    place = jnp.stack([y, fs, tp]).astype(jnp.int32)
    qa, kva, w_stick = stick_project(
        place, weights, [x, r1, l1, r2, l2], [other_y[0], other_r[0], other_l[0], other_r[1], other_l[1]]
    )
    kva_all = around("y", kva)
    qf, of, end = delta_local(
        place, decay_log_scale, write_bias, decay_w.T, write_w.T, weights, at_y, other_y, shifts
    )
    qb, kvb = stick_project(None, w_stick, [r3, l3, r4, l4], other_r[2:3] + other_l[2:3] + other_r[3:] + other_l[3:])
    kvb_all = around("y", kvb)
    ends = [
        functools.partial(lax.ppermute, axis_name=Z, perm=[(i, i + d) for i in range(8 - d)])(end)
        for d in range(7, 0, -1)
    ]
    dm = delta_finish(head_gain.reshape(1, 128), qf, of, ends)
    dm = lax.all_to_all(dm.reshape(8, 128, 128), ("y", "tp"), 0, 0, tiled=True)
    outs_other = [swap(sb_out_w), swap(delta_out_w)]

    u = jnp.asarray(np.tril(np.ones((CH, CH), np.float32), -1), bf16)
    sb = stick_attention(item(jnp.asarray(work_list()), 4 * z + y), sb_offset, qa, qb, u, kva_all + kvb_all)
    sb = lax.all_to_all(sb, (*Z, "tp"), 0, 0, tiled=True)

    sb = sb.reshape(8, 2, 64, 2, 64).transpose(1, 3, 2, 0, 4).reshape(2, 128, 512)
    dm = dm.reshape(4, 2, 128, 128).transpose(1, 2, 0, 3).reshape(2, 128, 512)

    def out_rows(rows, own_w, other_w):
        return jnp.dot(item(rows, tp), own_w, preferred_element_type=f32) + jnp.dot(
            item(rows, 1 - tp), other_w, preferred_element_type=f32
        )

    out = out_rows(dm, delta_out_w, outs_other[1])
    out = out + out_rows(sb, sb_out_w, outs_other[0])
    return out.astype(bf16).reshape(1, 128, 2048)


def solution(mesh):
    finer = Mesh(mesh.devices.reshape(2, 4, 4, mesh.shape["fs"], mesh.shape["tp"]), AXES)
    sp = ("zh", "zl", "y")
    return jax.shard_map(
        on_device,
        mesh=finer,
        in_specs=(
            P("fs", sp, "tp"),
            P("fs", "tp"),
            P("fs", "tp"),
            P("fs", "tp"),
            P("tp"),
            P("fs", "tp"),
            P("fs", "tp"),
            P("fs", "tp"),
            P(None, "tp"),
            P(None, "tp"),
            P("tp"),
            P("tp"),
            P("fs", "tp", sp),
            P(),
            P("tp", None),
            P("tp", None),
        ),
        out_specs=P("fs", (*sp, "tp"), None),
        check_vma=False,
    )
```

```python
import functools

import jax
import jax.numpy as jnp
import numpy as np
from jax import lax
from jax.experimental import pallas as pl
from jax.experimental.pallas import tpu as pltpu
from jax.sharding import Mesh
from jax.sharding import PartitionSpec as P


f32 = jnp.float32
bf16 = jnp.bfloat16
LOG2E = float(np.log2(np.e))
EPS = 1e-6
CH = 256
NT = (((1,), (1,)), ((), ()))
Z = ("zh", "zl")
AXES = ("zh", "zl", "y", "fs", "tp")


SLOT = (0, 2, 4, 6, 7, 5, 3, 1)
PAIRS, SINGLE, SLOTS, COUNT, HEAD = 0, 256, 320, 328, 329


def work_list():
    table = np.zeros((32, 384), np.int32)
    for z in range(8):
        slot = lambda i: SLOT[(i - z) % 8]
        for y in range(4):
            row = table[4 * z + y]
            place = lambda i, m: (m % 4) * 8 + slot((4 * i + y - m) // 4)
            steps = [(slot(2 * p), slot(2 * p + 1), place(2 * p, m)) for p in (3, 2, 1, 0) for m in range(1, 8 * p + y + 1)]
            for n, step in enumerate(steps):
                for k in range(3):
                    row[PAIRS + 64 * k + n] = step[k]
            for chain, ps in enumerate(((3, 1), (2, 0))):
                steps_one = [(slot(2 * p + 1), place(2 * p + 1, m)) for p in ps for m in range(1, 5)]
                for n, step in enumerate(steps_one):
                    row[SINGLE + 16 * chain + n] = step[0]
                    row[SINGLE + 16 * chain + 8 + n] = step[1]
            row[SLOTS : SLOTS + 8] = [slot(i) for i in range(8)]
            row[COUNT], row[HEAD] = len(steps), z
    return table


def stick_kernel(table, off_ref, q, u_ref, *refs):
    kv_refs, o_ref, (acc, run, kvs, kt, late_a, late_b, sp_a, sp_b) = refs[:4], refs[4], refs[5:]
    off = off_ref[table[HEAD]] * LOG2E
    for d in range(4):
        for n in range(8):
            block = kv_refs[d][n]
            kvs[d * 8 + n] = block
            kt[d * 8 + n] = jnp.transpose(block)

    def tile(slots, c, masked):
        size = CH * len(slots)
        join = lambda ref: jnp.concatenate([ref[s] for s in slots], axis=0) if len(slots) > 1 else ref[slots[0]]
        kv = kvs[c]
        z = jnp.dot(join(q), kt[c], preferred_element_type=f32) * (0.125 * LOG2E) + off
        sp = jnp.maximum(jnp.log2(1.0 + jnp.exp2(jnp.minimum(z, 40.0))), z)
        if masked:
            shape = (size, CH)
            seen = lax.broadcasted_iota(jnp.int32, shape, 1) < lax.broadcasted_iota(jnp.int32, shape, 0)
            sp = jnp.where(seen, sp, 0.0)
        after = jnp.dot(sp.astype(bf16), u_ref[...], preferred_element_type=f32)
        total = after[:, :1] + sp[:, :1]
        if masked:
            w = jnp.where(seen, jnp.exp2((z - sp) - after), 0.0)
            total = jnp.broadcast_to(total, (size, 128))
            out = jnp.dot(w.astype(bf16), kv, preferred_element_type=f32)
        else:
            r = join(run)
            w = jnp.exp2((z - sp) - (after + jnp.concatenate([r, r], axis=1)))
            total = r + total
            out = join(acc) + jnp.dot(w.astype(bf16), kv, preferred_element_type=f32)
        for k, s in enumerate(slots):
            run[s] = total[k * CH : k * CH + CH]
            acc[s] = out[k * CH : k * CH + CH]

    def diagonal(n, carry):
        for k in range(2):
            tile((2 * n + k,), 2 * n + k, True)
        return carry

    lax.fori_loop(0, 4, diagonal, 0)

    def one(n, carry):
        for k in range(2):
            tile((table[SINGLE + 16 * k + n],), table[SINGLE + 16 * k + 8 + n], False)
        return carry

    lax.fori_loop(0, 8, one, 0)

    def step(n):
        return (table[PAIRS + n], table[PAIRS + 64 + n]), table[PAIRS + 128 + n]

    def scores(n, late, sp_at):
        slots, c = step(n)
        z = jnp.dot(jnp.concatenate([q[s] for s in slots]), kt[c], preferred_element_type=f32) * (0.125 * LOG2E) + off
        sp = jnp.maximum(jnp.log2(1.0 + jnp.exp2(jnp.minimum(z, 40.0))), z)
        late[...] = z - sp
        sp_at[...] = sp.astype(bf16)

    def weigh(n, late, sp_at):
        slots, c = step(n)
        after = jnp.dot(sp_at[...], u_ref[...], preferred_element_type=f32)
        r = jnp.concatenate([run[s] for s in slots])
        w = jnp.exp2(late[...] - (after + jnp.concatenate([r, r], axis=1)))
        out = jnp.dot(w.astype(bf16), kvs[c], preferred_element_type=f32)
        total = r + (after[:, :1] + sp_at[:, :1].astype(f32))
        for k, s in enumerate(slots):
            rows = slice(k * CH, k * CH + CH)
            run[s] = total[rows]
            acc[s] += out[rows]

    scores(0, late_a, sp_a)

    def two(m, carry):
        weigh(2 * m, late_a, sp_a)
        scores(2 * m + 1, late_b, sp_b)
        weigh(2 * m + 1, late_b, sp_b)
        scores(2 * m + 2, late_a, sp_a)
        return carry

    lax.fori_loop(0, table[COUNT] // 2, two, 0)
    lane = lax.broadcasted_iota(jnp.int32, (64, 128), 1)
    for i in range(8):
        rows = acc[table[SLOTS + i]]
        for h in range(2):
            low, high = rows[128 * h : 128 * h + 64], rows[128 * h + 64 : 128 * h + 128]
            o_ref[2 * i + h] = jnp.where(lane < 64, pltpu.roll(low, 64, 1), high).astype(bf16)


def stick_attention(table, off, q, u, kvs):
    smem = pl.BlockSpec(memory_space=pltpu.SMEM)
    vmem = pl.BlockSpec(memory_space=pltpu.VMEM)
    return pl.pallas_call(
        stick_kernel,
        out_shape=jax.ShapeDtypeStruct((16, 64, 128), bf16),
        in_specs=[smem] * 2 + [vmem] * 6,
        out_specs=vmem,
        scratch_shapes=[
            pltpu.VMEM((8, CH, 128), f32),
            pltpu.VMEM((8, CH, 128), f32),
            pltpu.VMEM((32, CH, 128), bf16),
            pltpu.VMEM((32, 128, CH), bf16),
            pltpu.VMEM((2 * CH, CH), f32),
            pltpu.VMEM((2 * CH, CH), f32),
            pltpu.VMEM((2 * CH, CH), bf16),
            pltpu.VMEM((2 * CH, CH), bf16),
        ],
        cost_estimate=pl.CostEstimate(flops=20_000_000_000, bytes_accessed=4_000_000, transcendentals=26_000_000),
        name="stick_attention",
    )(table, off, q, u, *kvs)


def fetch(own, other, x_all, sems):
    copies = []
    for h, pieces in enumerate((own, other)):
        at = 0
        for k, piece in enumerate(pieces):
            rows = piece.shape[0]
            to = x_all.at[at // CH, pl.ds(at % CH, rows), pl.ds(h * 1024, 1024)]
            copy = pltpu.make_async_copy(piece, to, sems.at[h, k])
            copy.start()
            copies.append(copy)
            at += rows
    return copies


def project_rows(w_copies, copies, one, x_all, sems, w_ref, q_ref, kv_ref):
    for copy in w_copies:
        copy.wait()
    halves = len(copies) // 2

    def chunk(n):
        out = jnp.dot(x_all[n], w_ref[...], preferred_element_type=f32).astype(bf16)
        q_ref[n] = out[:, :128]
        kv_ref[n] = out[:, 128:]

    def whole(n, carry):
        for h in range(2):
            pltpu.make_async_copy(one, x_all.at[n, :, pl.ds(h * 1024, 1024)], sems.at[h, n]).wait()
        chunk(n)
        return carry

    lax.fori_loop(0, 7, whole, 0)
    for k in (7, 8, halves + 7, halves + 8):
        copies[k].wait()
    chunk(7)


def fetch_weights(place, pieces, columns, w_all, sems):
    copies = []
    for d, piece in enumerate(pieces):
        at = lax.rem(place[1] - d - 2 * place[2] + 8, 4)
        to = w_all.at[pl.ds(pl.multiple_of(at * 512, 512), 512), :]
        copy = pltpu.make_async_copy(piece.at[:, columns], to, sems.at[d])
        copy.start()
        copies.append(copy)
    return copies


def project_kernel(place, *refs):
    weights, x, (q_ref, kv_ref, w_all, x_all, sems, w_sems) = refs[:4], refs[4:-6], refs[-6:]
    half = len(x) // 2
    w_copies = fetch_weights(place, weights, pl.ds(0, 256), w_all, w_sems)
    copies = fetch(x[:half], x[half:], x_all, sems)
    project_rows(w_copies, copies, x[0], x_all, sems, w_all, q_ref, kv_ref)


def stick_project(place, weights, own, other):
    vmem = pl.BlockSpec(memory_space=pltpu.VMEM)
    anywhere = pl.BlockSpec(memory_space=pl.ANY)
    shape = jax.ShapeDtypeStruct((8, CH, 128), bf16)
    return pl.pallas_call(
        project_kernel,
        out_shape=(shape, shape),
        in_specs=[pl.BlockSpec(memory_space=pltpu.SMEM)] + [anywhere] * (4 + len(own) + len(other)),
        out_specs=(vmem, vmem),
        scratch_shapes=[
            pltpu.VMEM((2048, 256), bf16),
            pltpu.VMEM((8, CH, 2048), bf16),
            pltpu.SemaphoreType.DMA((2, len(own))),
            pltpu.SemaphoreType.DMA((4,)),
        ],
        cost_estimate=pl.CostEstimate(flops=2_200_000_000, bytes_accessed=10_000_000, transcendentals=0),
        name="stick_project",
    )(place, *weights, *own, *other)


def mm(a, b, dims=(((1,), (0,)), ((), ()))):
    return lax.dot_general(a.astype(bf16), b.astype(bf16), dims, preferred_element_type=f32)


def silu(u):
    return u * jax.nn.sigmoid(u)


def unit(u):
    return u * lax.rsqrt(jnp.sum(u * u, axis=-1, keepdims=True) + EPS)


def delta_kernel(place, scale_ref, bias_ref, decay_ref, write_ref, *refs):
    shifts, weights, own, other = refs[:4], refs[4:8], refs[8:12], refs[12:16]
    qf_ref, of_ref, end_ref, x_all, w_all, side_w, proj_all, maps, addend, rows_all, sems, w_sems = refs[16:]
    y, tp = place[0], place[2]
    w_copies = fetch_weights(place, weights, pl.ds(256, 384), w_all, w_sems)
    fetch(own, other, x_all, sems)
    minus_scale = -jnp.exp(jnp.full((CH, 1), scale_ref[y], f32))
    bias = bias_ref[y]
    for h in range(2):
        at = pl.ds(pl.multiple_of((tp if h == 0 else 1 - tp) * 1024, 1024), 1024)
        side_w[:, h * 1024 : h * 1024 + 1024] = jnp.concatenate([decay_ref[:, at], write_ref[:, at]], axis=0)
    lanes = lax.broadcasted_iota(jnp.int32, (CH, 128), 1)
    for d in range(4):
        proj_all[lax.rem(y - d + 4, 4), :, 384:] = jnp.transpose(jnp.broadcast_to(shifts[d][pl.ds(y, 1), :], (128, CH)))
    for copy in w_copies:
        copy.wait()
    narrow = lax.broadcasted_iota(jnp.int32, (CH, 8), 1)

    def project(d, carry):
        for h in range(2):
            pltpu.make_async_copy(own[0], x_all.at[d, :, pl.ds(h * 1024, 1024)], sems.at[h, d]).wait()
        x = x_all[d]
        at = lax.rem(y - d + 4, 4)
        proj_all[at, :, :384] = jnp.dot(x, w_all[...], preferred_element_type=f32)
        pre = lax.dot_general(x, side_w[...], NT, preferred_element_type=f32)
        decay_pre = jnp.sum(jnp.where(narrow == y, pre, 0.0), axis=1, keepdims=True)
        write_pre = jnp.sum(jnp.where(narrow == y + 4, pre, 0.0), axis=1, keepdims=True)
        proj_all[at, :, 384:] = jnp.where(lanes == 0, decay_pre, jnp.where(lanes == 1, write_pre, proj_all[at, :, 384:]))
        return carry

    lax.fori_loop(0, 4, project, 0)
    span = (CH, CH)
    row = lax.broadcasted_iota(jnp.int32, span, 0)
    col = lax.broadcasted_iota(jnp.int32, span, 1)
    same = (row // 64) == (col // 64)
    inclusive = jnp.logical_and(same, col <= row)
    strict = jnp.logical_and(same, col < row)
    sums = jnp.concatenate([jnp.where(inclusive, 1.0, 0.0), jnp.where(same, 1.0, 0.0)], axis=0)
    eye = jnp.where(row == col, 1.0, 0.0)
    wide = lax.broadcasted_iota(jnp.int32, (128, CH), 1) // 64
    small_eye = jnp.where(
        lax.broadcasted_iota(jnp.int32, (128, 128), 0) == lax.broadcasted_iota(jnp.int32, (128, 128), 1), 1.0, 0.0
    )

    def blocks(m, carry):
        tiles = range(2)
        cum, tot, q, k, v, beta = [], [], [], [], [], []
        for t in tiles:
            proj = proj_all[2 * m + t]
            dq, dk, dv = (proj[:, 128 * n : 128 * n + 128].astype(bf16).astype(f32) for n in range(3))
            pre = proj[:, 384:385]
            softplus = jnp.maximum(pre, 0.0) + jnp.log1p(jnp.exp(-jnp.abs(pre)))
            g = minus_scale * softplus + proj[:, 386:387]
            beta.append(jax.nn.sigmoid(proj[:, 385:386] + bias))
            q.append(unit(silu(dq)) * 128**-0.5)
            k.append(unit(silu(dk)))
            v.append(silu(dv))
            g1 = g.astype(bf16).astype(f32)
            g2 = (g - g1).astype(bf16).astype(f32)
            g3 = g - g1 - g2
            parts = jnp.where(lanes == 0, g1, jnp.where(lanes == 1, g2, jnp.where(lanes == 2, g3, 0.0)))
            s = mm(sums, parts)
            s = jnp.broadcast_to(s[:, 0:1] + s[:, 1:2] + s[:, 2:3], (2 * CH, 128))
            cum.append(s[:CH])
            tot.append(s[CH:])
        table = []
        for t in tiles:
            across = jnp.transpose(cum[t])[0:1, :]
            spread = cum[t][:, 0:1] - across
            table.append(jnp.where(inclusive, jnp.exp(jnp.where(inclusive, spread, 0.0)), 0.0))
        keys_beta = [k[t] * beta[t] for t in tiles]
        power = [jnp.where(strict, mm(keys_beta[t], k[t], NT) * table[t], 0.0) for t in tiles]
        inside = [mm(q[t], k[t], NT) * table[t] for t in tiles]
        inverse = [eye - power[t] for t in tiles]
        for _ in range(5):
            power = [mm(power[t], power[t]) for t in tiles]
            inverse = [inverse[t] + mm(inverse[t], power[t]) for t in tiles]
        growth = [jnp.exp(cum[t]) for t in tiles]
        both = [
            mm(inverse[t], jnp.concatenate([keys_beta[t] * growth[t], v[t] * beta[t]], axis=1)) for t in tiles
        ]
        seen = [mm(inside[t], both[t]) for t in tiles]
        for t in tiles:
            n0 = 4 * (2 * m + t)
            reach = q[t] * growth[t] - seen[t][:, :128]
            damped = jnp.transpose(k[t] * jnp.exp(tot[t] - cum[t]))
            moved = mm(jnp.concatenate([jnp.where(wide == b, damped, 0.0) for b in range(4)], axis=0), both[t])
            for b in range(4):
                decay = jnp.exp(tot[t][b * 64 : b * 64 + 1, :])
                piece = moved[b * 128 : b * 128 + 128]
                maps[n0 + b, :64] = reach[b * 64 : b * 64 + 64].astype(bf16)
                maps[n0 + b, 64:] = (small_eye * decay - piece[:, :128]).astype(bf16)
                addend[n0 + b, :64] = seen[t][b * 64 : b * 64 + 64, 128:]
                addend[n0 + b, 64:] = piece[:, 128:]
        return carry

    lax.fori_loop(0, 2, blocks, 0)
    rows_all[...] = jnp.concatenate([small_eye, jnp.zeros((128, 128), f32)], axis=1)

    def chain(n, carry):
        moved = jnp.dot(maps[n], rows_all[...].astype(bf16), preferred_element_type=f32)
        after = moved[:, 128:] + addend[n]
        at = pl.ds(pl.multiple_of(n * 64, 64), 64)
        qf_ref[at, :] = moved[:64, :128]
        of_ref[at, :] = after[:64]
        rows_all[...] = jnp.concatenate([moved[64:, :128], after[64:]], axis=1)
        return carry

    lax.fori_loop(0, 16, chain, 0)
    end_ref[...] = rows_all[...].astype(bf16)


def delta_local(place, scale, bias, decay_w, write_w, weights, own, other, shifts):
    smem = pl.BlockSpec(memory_space=pltpu.SMEM)
    vmem = pl.BlockSpec(memory_space=pltpu.VMEM)
    return pl.pallas_call(
        delta_kernel,
        out_shape=(
            jax.ShapeDtypeStruct((1024, 128), f32),
            jax.ShapeDtypeStruct((1024, 128), f32),
            jax.ShapeDtypeStruct((128, 256), bf16),
        ),
        in_specs=[smem] * 3 + [vmem] * 6 + [pl.BlockSpec(memory_space=pl.ANY)] * 12,
        out_specs=(vmem,) * 3,
        scratch_shapes=[
            pltpu.VMEM((4, CH, 2048), bf16),
            pltpu.VMEM((2048, 384), bf16),
            pltpu.VMEM((8, 2048), bf16),
            pltpu.VMEM((4, CH, 512), f32),
            pltpu.VMEM((16, 192, 128), bf16),
            pltpu.VMEM((16, 192, 128), f32),
            pltpu.VMEM((128, 256), f32),
            pltpu.SemaphoreType.DMA((2, 4)),
            pltpu.SemaphoreType.DMA((4,)),
        ],
        cost_estimate=pl.CostEstimate(flops=12_000_000_000, bytes_accessed=8_000_000, transcendentals=1_000_000),
        name="delta_local",
    )(place, scale, bias, decay_w, write_w, *shifts, *weights, *own, *other)


def finish_kernel(gain_ref, qf_ref, of_ref, *refs):
    maps, o_ref = refs[:-1], refs[-1]
    state = jnp.zeros((128, 128), f32)
    for ref in maps:
        state = mm(ref[:, :128], state) + ref[:, 128:].astype(f32)
    for t in range(4):
        rows = slice(t * CH, (t + 1) * CH)
        o = mm(qf_ref[rows, :], state) + of_ref[rows, :]
        o = o * lax.rsqrt(jnp.mean(o * o, axis=-1, keepdims=True) + EPS) * gain_ref[...]
        o_ref[rows, :] = o.astype(bf16)


def delta_finish(gain, qf, of, maps):
    vmem = pl.BlockSpec(memory_space=pltpu.VMEM)
    return pl.pallas_call(
        finish_kernel,
        out_shape=jax.ShapeDtypeStruct((1024, 128), bf16),
        in_specs=[vmem] * (3 + len(maps)),
        out_specs=vmem,
        cost_estimate=pl.CostEstimate(flops=1_000_000_000, bytes_accessed=2_000_000, transcendentals=2_000),
        name="delta_finish",
    )(gain, qf, of, *maps)


def ring(axis, size, step):
    return functools.partial(lax.ppermute, axis_name=axis, perm=[(i, (i + step) % size) for i in range(size)])


def on_device(
    hidden_in,
    sb_query_w,
    sb_key_w,
    sb_value_w,
    sb_offset,
    delta_query_w,
    delta_key_w,
    delta_value_w,
    decay_w,
    write_w,
    write_bias,
    decay_log_scale,
    decay_shift,
    head_gain,
    sb_out_w,
    delta_out_w,
):
    z, y, fs, tp = lax.axis_index(Z), lax.axis_index("y"), lax.axis_index("fs"), lax.axis_index("tp")
    x = hidden_in.reshape(256, 1024)

    across = functools.partial(lax.ppermute, axis_name="tp", perm=[(0, 1), (1, 0)])
    swap = lambda v: across(v)
    right, left = ring(Z, 8, 1), ring(Z, 8, 7)
    around = lambda axis, v: [v] + [ring(axis, 4, d)(v) for d in (1, 2, 3)]
    pick = lambda w, at, n: lax.dynamic_slice_in_dim(w, at, n, 1)
    item = lambda v, at: lax.dynamic_index_in_dim(v, at, 0, keepdims=False)

    mine = jnp.concatenate(
        [pick(sb_query_w, z * 64, 64), jnp.zeros((512, 64), bf16), pick(sb_key_w, z * 64, 64), pick(sb_value_w, z * 64, 64)]
        + [pick(w, y * 128, 128) for w in (delta_query_w, delta_key_w, delta_value_w)],
        axis=1,
    )
    r1, l1 = right(x), left(x)
    at_y = around("y", x)
    weights = around("fs", mine)
    r2, l2 = right(r1), left(l1)
    r3, l3 = right(r2), left(l2)
    r4, l4 = right(r3[:128]), left(l3[128:])
    other_y = [swap(v) for v in at_y]
    other_r = [swap(v) for v in (r1, r2, r3, r4)]
    other_l = [swap(v) for v in (l1, l2, l3, l4)]
    shifts = around("y", decay_shift.reshape(4, 256))

    place = jnp.stack([y, fs, tp]).astype(jnp.int32)
    q, kv = stick_project(
        place,
        weights,
        [x, r1, l1, r2, l2, r3, l3, r4, l4],
        [other_y[0]] + [v for pair in zip(other_r, other_l) for v in pair],
    )
    kvs = around("y", kv)
    qf, of, end = delta_local(
        place, decay_log_scale, write_bias, decay_w.T, write_w.T, weights, at_y, other_y, shifts
    )
    ends = [
        functools.partial(lax.ppermute, axis_name=Z, perm=[(i, i + d) for i in range(8 - d)])(end)
        for d in range(7, 0, -1)
    ]
    dm = delta_finish(head_gain.reshape(1, 128), qf, of, ends)
    dm = lax.all_to_all(dm.reshape(8, 128, 128), ("y", "tp"), 0, 0, tiled=True)
    outs_other = [swap(sb_out_w), swap(delta_out_w)]

    u = jnp.asarray(np.tril(np.ones((CH, CH), np.float32), -1), bf16)
    sb = stick_attention(item(jnp.asarray(work_list()), 4 * z + y), sb_offset, q, u, kvs)
    sb = lax.all_to_all(sb, (*Z, "tp"), 0, 0, tiled=True)

    sb = sb.reshape(8, 2, 64, 2, 64).transpose(1, 3, 2, 0, 4).reshape(2, 128, 512)
    dm = dm.reshape(4, 2, 128, 128).transpose(1, 2, 0, 3).reshape(2, 128, 512)

    def out_rows(rows, own_w, other_w):
        return jnp.dot(item(rows, tp), own_w, preferred_element_type=f32) + jnp.dot(
            item(rows, 1 - tp), other_w, preferred_element_type=f32
        )

    out = out_rows(dm, delta_out_w, outs_other[1])
    out = out + out_rows(sb, sb_out_w, outs_other[0])
    return out.astype(bf16).reshape(1, 128, 2048)


def solution(mesh):
    finer = Mesh(mesh.devices.reshape(2, 4, 4, mesh.shape["fs"], mesh.shape["tp"]), AXES)
    sp = ("zh", "zl", "y")
    return jax.shard_map(
        on_device,
        mesh=finer,
        in_specs=(
            P("fs", sp, "tp"),
            P("fs", "tp"),
            P("fs", "tp"),
            P("fs", "tp"),
            P("tp"),
            P("fs", "tp"),
            P("fs", "tp"),
            P("fs", "tp"),
            P(None, "tp"),
            P(None, "tp"),
            P("tp"),
            P("tp"),
            P("fs", "tp", sp),
            P(),
            P("tp", None),
            P("tp", None),
        ),
        out_specs=P("fs", (*sp, "tp"), None),
        check_vma=False,
    )
```

```python
import functools

import jax
import jax.numpy as jnp
import numpy as np
from jax import lax
from jax.experimental import pallas as pl
from jax.experimental.pallas import tpu as pltpu
from jax.sharding import Mesh
from jax.sharding import PartitionSpec as P


f32 = jnp.float32
bf16 = jnp.bfloat16
LOG2E = float(np.log2(np.e))
EPS = 1e-6
CH = 256
NT = (((1,), (1,)), ((), ()))
Z = ("zh", "zl")
AXES = ("zh", "zl", "y", "fs", "tp")


SLOT = (0, 2, 4, 6, 7, 5, 3, 1)
PAIRS, SINGLE, SLOTS, COUNT, HEAD = 0, 256, 320, 328, 329


def work_list():
    table = np.zeros((32, 384), np.int32)
    for z in range(8):
        slot = lambda i: SLOT[(i - z) % 8]
        for y in range(4):
            row = table[4 * z + y]
            place = lambda i, m: (m % 4) * 8 + slot((4 * i + y - m) // 4)
            steps = [(slot(2 * p), slot(2 * p + 1), place(2 * p, m)) for p in (3, 2, 1, 0) for m in range(1, 8 * p + y + 1)]
            for n, step in enumerate(steps):
                for k in range(3):
                    row[PAIRS + 64 * k + n] = step[k]
            for chain, ps in enumerate(((3, 1), (2, 0))):
                steps_one = [(slot(2 * p + 1), place(2 * p + 1, m)) for p in ps for m in range(1, 5)]
                for n, step in enumerate(steps_one):
                    row[SINGLE + 16 * chain + n] = step[0]
                    row[SINGLE + 16 * chain + 8 + n] = step[1]
            row[SLOTS : SLOTS + 8] = [slot(i) for i in range(8)]
            row[COUNT], row[HEAD] = len(steps), z
    return table


def stick_kernel(table, off_ref, q, u_ref, *refs):
    kv_refs, o_ref, (acc, run, kvs, kt, late_a, late_b, sp_a, sp_b) = refs[:4], refs[4], refs[5:]
    off = off_ref[table[HEAD]] * LOG2E
    for d in range(4):
        for n in range(8):
            block = kv_refs[d][n]
            kvs[d * 8 + n] = block
            kt[d * 8 + n] = jnp.transpose(block)

    def tile(slots, c, masked):
        size = CH * len(slots)
        join = lambda ref: jnp.concatenate([ref[s] for s in slots], axis=0) if len(slots) > 1 else ref[slots[0]]
        kv = kvs[c]
        z = jnp.dot(join(q), kt[c], preferred_element_type=f32) * (0.125 * LOG2E) + off
        sp = jnp.maximum(jnp.log2(1.0 + jnp.exp2(jnp.minimum(z, 40.0))), z)
        if masked:
            shape = (size, CH)
            seen = lax.broadcasted_iota(jnp.int32, shape, 1) < lax.broadcasted_iota(jnp.int32, shape, 0)
            sp = jnp.where(seen, sp, 0.0)
        after = jnp.dot(sp.astype(bf16), u_ref[...], preferred_element_type=f32)
        total = after[:, :1] + sp[:, :1]
        if masked:
            w = jnp.where(seen, jnp.exp2((z - sp) - after), 0.0)
            total = jnp.broadcast_to(total, (size, 128))
            out = jnp.dot(w.astype(bf16), kv, preferred_element_type=f32)
        else:
            r = join(run)
            w = jnp.exp2((z - sp) - (after + jnp.concatenate([r, r], axis=1)))
            total = r + total
            out = join(acc) + jnp.dot(w.astype(bf16), kv, preferred_element_type=f32)
        for k, s in enumerate(slots):
            run[s] = total[k * CH : k * CH + CH]
            acc[s] = out[k * CH : k * CH + CH]

    def diagonal(n, carry):
        for k in range(2):
            tile((2 * n + k,), 2 * n + k, True)
        return carry

    lax.fori_loop(0, 4, diagonal, 0)

    def one(n, carry):
        for k in range(2):
            tile((table[SINGLE + 16 * k + n],), table[SINGLE + 16 * k + 8 + n], False)
        return carry

    lax.fori_loop(0, 8, one, 0)

    def step(n):
        return (table[PAIRS + n], table[PAIRS + 64 + n]), table[PAIRS + 128 + n]

    def scores(n, late, sp_at):
        slots, c = step(n)
        z = jnp.dot(jnp.concatenate([q[s] for s in slots]), kt[c], preferred_element_type=f32) * (0.125 * LOG2E) + off
        sp = jnp.maximum(jnp.log2(1.0 + jnp.exp2(jnp.minimum(z, 40.0))), z)
        late[...] = z - sp
        sp_at[...] = sp.astype(bf16)

    def weigh(n, late, sp_at):
        slots, c = step(n)
        after = jnp.dot(sp_at[...], u_ref[...], preferred_element_type=f32)
        r = jnp.concatenate([run[s] for s in slots])
        w = jnp.exp2(late[...] - (after + jnp.concatenate([r, r], axis=1)))
        out = jnp.dot(w.astype(bf16), kvs[c], preferred_element_type=f32)
        total = r + (after[:, :1] + sp_at[:, :1].astype(f32))
        for k, s in enumerate(slots):
            rows = slice(k * CH, k * CH + CH)
            run[s] = total[rows]
            acc[s] += out[rows]

    scores(0, late_a, sp_a)

    def two(m, carry):
        weigh(2 * m, late_a, sp_a)
        scores(2 * m + 1, late_b, sp_b)
        weigh(2 * m + 1, late_b, sp_b)
        scores(2 * m + 2, late_a, sp_a)
        return carry

    lax.fori_loop(0, table[COUNT] // 2, two, 0)
    lane = lax.broadcasted_iota(jnp.int32, (64, 128), 1)
    for i in range(8):
        rows = acc[table[SLOTS + i]]
        for h in range(2):
            low, high = rows[128 * h : 128 * h + 64], rows[128 * h + 64 : 128 * h + 128]
            o_ref[2 * i + h] = jnp.where(lane < 64, pltpu.roll(low, 64, 1), high).astype(bf16)


def stick_attention(table, off, q, u, kvs):
    smem = pl.BlockSpec(memory_space=pltpu.SMEM)
    vmem = pl.BlockSpec(memory_space=pltpu.VMEM)
    return pl.pallas_call(
        stick_kernel,
        out_shape=jax.ShapeDtypeStruct((16, 64, 128), bf16),
        in_specs=[smem] * 2 + [vmem] * 6,
        out_specs=vmem,
        scratch_shapes=[
            pltpu.VMEM((8, CH, 128), f32),
            pltpu.VMEM((8, CH, 128), f32),
            pltpu.VMEM((32, CH, 128), bf16),
            pltpu.VMEM((32, 128, CH), bf16),
            pltpu.VMEM((2 * CH, CH), f32),
            pltpu.VMEM((2 * CH, CH), f32),
            pltpu.VMEM((2 * CH, CH), bf16),
            pltpu.VMEM((2 * CH, CH), bf16),
        ],
        cost_estimate=pl.CostEstimate(flops=20_000_000_000, bytes_accessed=4_000_000, transcendentals=26_000_000),
        name="stick_attention",
    )(table, off, q, u, *kvs)


def fetch(own, other, x_all, sems):
    copies = []
    for h, pieces in enumerate((own, other)):
        at = 0
        for k, piece in enumerate(pieces):
            rows = piece.shape[0]
            to = x_all.at[at // CH, pl.ds(at % CH, rows), pl.ds(h * 1024, 1024)]
            copy = pltpu.make_async_copy(piece, to, sems.at[h, k])
            copy.start()
            copies.append(copy)
            at += rows
    return copies


def project_rows(w_copies, copies, one, x_all, sems, w_ref, q_ref, kv_ref):
    for copy in w_copies:
        copy.wait()
    halves = len(copies) // 2

    def chunk(n):
        out = jnp.dot(x_all[n], w_ref[...], preferred_element_type=f32).astype(bf16)
        q_ref[n] = out[:, :128]
        kv_ref[n] = out[:, 128:]

    def whole(n, carry):
        for h in range(2):
            pltpu.make_async_copy(one, x_all.at[n, :, pl.ds(h * 1024, 1024)], sems.at[h, n]).wait()
        chunk(n)
        return carry

    lax.fori_loop(0, 7, whole, 0)
    for k in (7, 8, halves + 7, halves + 8):
        copies[k].wait()
    chunk(7)


def fetch_weights(place, pieces, columns, w_all, sems):
    copies = []
    for d, piece in enumerate(pieces):
        at = lax.rem(place[1] - d - 2 * place[2] + 8, 4)
        to = w_all.at[pl.ds(pl.multiple_of(at * 512, 512), 512), :]
        copy = pltpu.make_async_copy(piece.at[:, columns], to, sems.at[d])
        copy.start()
        copies.append(copy)
    return copies


def project_kernel(place, *refs):
    weights, x, (q_ref, kv_ref, w_all, x_all, sems, w_sems) = refs[:4], refs[4:-6], refs[-6:]
    half = len(x) // 2
    w_copies = fetch_weights(place, weights, pl.ds(0, 256), w_all, w_sems)
    copies = fetch(x[:half], x[half:], x_all, sems)
    project_rows(w_copies, copies, x[0], x_all, sems, w_all, q_ref, kv_ref)


def stick_project(place, weights, own, other):
    vmem = pl.BlockSpec(memory_space=pltpu.VMEM)
    anywhere = pl.BlockSpec(memory_space=pl.ANY)
    shape = jax.ShapeDtypeStruct((8, CH, 128), bf16)
    return pl.pallas_call(
        project_kernel,
        out_shape=(shape, shape),
        in_specs=[pl.BlockSpec(memory_space=pltpu.SMEM)] + [anywhere] * (4 + len(own) + len(other)),
        out_specs=(vmem, vmem),
        scratch_shapes=[
            pltpu.VMEM((2048, 256), bf16),
            pltpu.VMEM((8, CH, 2048), bf16),
            pltpu.SemaphoreType.DMA((2, len(own))),
            pltpu.SemaphoreType.DMA((4,)),
        ],
        cost_estimate=pl.CostEstimate(flops=2_200_000_000, bytes_accessed=10_000_000, transcendentals=0),
        name="stick_project",
    )(place, *weights, *own, *other)


def mm(a, b, dims=(((1,), (0,)), ((), ()))):
    return lax.dot_general(a.astype(bf16), b.astype(bf16), dims, preferred_element_type=f32)


def silu(u):
    return u * jax.nn.sigmoid(u)


def unit(u):
    return u * lax.rsqrt(jnp.sum(u * u, axis=-1, keepdims=True) + EPS)


def delta_kernel(place, scale_ref, bias_ref, decay_ref, write_ref, *refs):
    shifts, weights, own, other = refs[:4], refs[4:8], refs[8:12], refs[12:16]
    qf_ref, of_ref, end_ref, x_all, w_all, side_w, proj_all, maps, addend, rows_all, sems, w_sems = refs[16:]
    y, tp = place[0], place[2]
    w_copies = fetch_weights(place, weights, pl.ds(256, 384), w_all, w_sems)
    fetch(own, other, x_all, sems)
    minus_scale = -jnp.exp(jnp.full((CH, 1), scale_ref[y], f32))
    bias = bias_ref[y]
    for h in range(2):
        at = pl.ds(pl.multiple_of((tp if h == 0 else 1 - tp) * 1024, 1024), 1024)
        side_w[:, h * 1024 : h * 1024 + 1024] = jnp.concatenate([decay_ref[:, at], write_ref[:, at]], axis=0)
    lanes = lax.broadcasted_iota(jnp.int32, (CH, 128), 1)
    for d in range(4):
        proj_all[lax.rem(y - d + 4, 4), :, 384:] = jnp.transpose(jnp.broadcast_to(shifts[d][pl.ds(y, 1), :], (128, CH)))
    for copy in w_copies:
        copy.wait()
    narrow = lax.broadcasted_iota(jnp.int32, (CH, 8), 1)

    def project(d, carry):
        for h in range(2):
            pltpu.make_async_copy(own[0], x_all.at[d, :, pl.ds(h * 1024, 1024)], sems.at[h, d]).wait()
        x = x_all[d]
        at = lax.rem(y - d + 4, 4)
        proj_all[at, :, :384] = jnp.dot(x, w_all[...], preferred_element_type=f32)
        pre = lax.dot_general(x, side_w[...], NT, preferred_element_type=f32)
        decay_pre = jnp.sum(jnp.where(narrow == y, pre, 0.0), axis=1, keepdims=True)
        write_pre = jnp.sum(jnp.where(narrow == y + 4, pre, 0.0), axis=1, keepdims=True)
        proj_all[at, :, 384:] = jnp.where(lanes == 0, decay_pre, jnp.where(lanes == 1, write_pre, proj_all[at, :, 384:]))
        return carry

    lax.fori_loop(0, 4, project, 0)
    span = (CH, CH)
    row = lax.broadcasted_iota(jnp.int32, span, 0)
    col = lax.broadcasted_iota(jnp.int32, span, 1)
    same = (row // 64) == (col // 64)
    inclusive = jnp.logical_and(same, col <= row)
    strict = jnp.logical_and(same, col < row)
    sums = jnp.concatenate([jnp.where(inclusive, 1.0, 0.0), jnp.where(same, 1.0, 0.0)], axis=0)
    eye = jnp.where(row == col, 1.0, 0.0)
    wide = lax.broadcasted_iota(jnp.int32, (128, CH), 1) // 64
    small_eye = jnp.where(
        lax.broadcasted_iota(jnp.int32, (128, 128), 0) == lax.broadcasted_iota(jnp.int32, (128, 128), 1), 1.0, 0.0
    )

    def blocks(m, carry):
        tiles = range(2)
        cum, tot, q, k, v, beta = [], [], [], [], [], []
        for t in tiles:
            proj = proj_all[2 * m + t]
            dq, dk, dv = (proj[:, 128 * n : 128 * n + 128].astype(bf16).astype(f32) for n in range(3))
            pre = proj[:, 384:385]
            softplus = jnp.maximum(pre, 0.0) + jnp.log1p(jnp.exp(-jnp.abs(pre)))
            g = minus_scale * softplus + proj[:, 386:387]
            beta.append(jax.nn.sigmoid(proj[:, 385:386] + bias))
            q.append(unit(silu(dq)) * 128**-0.5)
            k.append(unit(silu(dk)))
            v.append(silu(dv))
            g1 = g.astype(bf16).astype(f32)
            g2 = (g - g1).astype(bf16).astype(f32)
            g3 = g - g1 - g2
            parts = jnp.where(lanes == 0, g1, jnp.where(lanes == 1, g2, jnp.where(lanes == 2, g3, 0.0)))
            s = mm(sums, parts)
            s = jnp.broadcast_to(s[:, 0:1] + s[:, 1:2] + s[:, 2:3], (2 * CH, 128))
            cum.append(s[:CH])
            tot.append(s[CH:])
        table = []
        for t in tiles:
            across = jnp.transpose(cum[t])[0:1, :]
            spread = cum[t][:, 0:1] - across
            table.append(jnp.where(inclusive, jnp.exp(jnp.where(inclusive, spread, 0.0)), 0.0))
        keys_beta = [k[t] * beta[t] for t in tiles]
        power = [jnp.where(strict, mm(keys_beta[t], k[t], NT) * table[t], 0.0) for t in tiles]
        inside = [mm(q[t], k[t], NT) * table[t] for t in tiles]
        inverse = [eye - power[t] for t in tiles]
        for _ in range(5):
            power = [mm(power[t], power[t]) for t in tiles]
            inverse = [inverse[t] + mm(inverse[t], power[t]) for t in tiles]
        growth = [jnp.exp(cum[t]) for t in tiles]
        both = [
            mm(inverse[t], jnp.concatenate([keys_beta[t] * growth[t], v[t] * beta[t]], axis=1)) for t in tiles
        ]
        seen = [mm(inside[t], both[t]) for t in tiles]
        for t in tiles:
            n0 = 4 * (2 * m + t)
            reach = q[t] * growth[t] - seen[t][:, :128]
            damped = jnp.transpose(k[t] * jnp.exp(tot[t] - cum[t]))
            moved = mm(jnp.concatenate([jnp.where(wide == b, damped, 0.0) for b in range(4)], axis=0), both[t])
            for b in range(4):
                decay = jnp.exp(tot[t][b * 64 : b * 64 + 1, :])
                piece = moved[b * 128 : b * 128 + 128]
                maps[n0 + b, :64] = reach[b * 64 : b * 64 + 64].astype(bf16)
                maps[n0 + b, 64:] = (small_eye * decay - piece[:, :128]).astype(bf16)
                addend[n0 + b, :64] = seen[t][b * 64 : b * 64 + 64, 128:]
                addend[n0 + b, 64:] = piece[:, 128:]
        return carry

    lax.fori_loop(0, 2, blocks, 0)
    rows_all[...] = jnp.concatenate([small_eye, jnp.zeros((128, 128), f32)], axis=1)

    def chain(n, carry):
        moved = jnp.dot(maps[n], rows_all[...].astype(bf16), preferred_element_type=f32)
        after = moved[:, 128:] + addend[n]
        at = pl.ds(pl.multiple_of(n * 64, 64), 64)
        qf_ref[at, :] = moved[:64, :128]
        of_ref[at, :] = after[:64]
        rows_all[...] = jnp.concatenate([moved[64:, :128], after[64:]], axis=1)
        return carry

    lax.fori_loop(0, 16, chain, 0)
    end_ref[...] = rows_all[...].astype(bf16)


def delta_local(place, scale, bias, decay_w, write_w, weights, own, other, shifts):
    smem = pl.BlockSpec(memory_space=pltpu.SMEM)
    vmem = pl.BlockSpec(memory_space=pltpu.VMEM)
    return pl.pallas_call(
        delta_kernel,
        out_shape=(
            jax.ShapeDtypeStruct((1024, 128), f32),
            jax.ShapeDtypeStruct((1024, 128), f32),
            jax.ShapeDtypeStruct((128, 256), bf16),
        ),
        in_specs=[smem] * 3 + [vmem] * 6 + [pl.BlockSpec(memory_space=pl.ANY)] * 12,
        out_specs=(vmem,) * 3,
        scratch_shapes=[
            pltpu.VMEM((4, CH, 2048), bf16),
            pltpu.VMEM((2048, 384), bf16),
            pltpu.VMEM((8, 2048), bf16),
            pltpu.VMEM((4, CH, 512), f32),
            pltpu.VMEM((16, 192, 128), bf16),
            pltpu.VMEM((16, 192, 128), f32),
            pltpu.VMEM((128, 256), f32),
            pltpu.SemaphoreType.DMA((2, 4)),
            pltpu.SemaphoreType.DMA((4,)),
        ],
        cost_estimate=pl.CostEstimate(flops=12_000_000_000, bytes_accessed=8_000_000, transcendentals=1_000_000),
        name="delta_local",
    )(place, scale, bias, decay_w, write_w, *shifts, *weights, *own, *other)


def finish_kernel(gain_ref, place, qf_ref, of_ref, maps, o_ref):
    state = jnp.zeros((128, 128), f32)
    for n in range(7):
        moved = mm(maps[n, :, :128], state) + maps[n, :, 128:].astype(f32)
        state = jnp.where(n < place[3], moved, state)
    for t in range(4):
        rows = slice(t * CH, (t + 1) * CH)
        o = mm(qf_ref[rows, :], state) + of_ref[rows, :]
        o = o * lax.rsqrt(jnp.mean(o * o, axis=-1, keepdims=True) + EPS) * gain_ref[...]
        o_ref[rows, :] = o.astype(bf16)


def delta_finish(gain, place, qf, of, maps):
    vmem = pl.BlockSpec(memory_space=pltpu.VMEM)
    return pl.pallas_call(
        finish_kernel,
        out_shape=jax.ShapeDtypeStruct((1024, 128), bf16),
        in_specs=[vmem, pl.BlockSpec(memory_space=pltpu.SMEM), vmem, vmem, vmem],
        out_specs=vmem,
        cost_estimate=pl.CostEstimate(flops=1_000_000_000, bytes_accessed=2_000_000, transcendentals=2_000),
        name="delta_finish",
    )(gain, place, qf, of, maps)


def ring(axis, size, step):
    return functools.partial(lax.ppermute, axis_name=axis, perm=[(i, (i + step) % size) for i in range(size)])


def on_device(
    hidden_in,
    sb_query_w,
    sb_key_w,
    sb_value_w,
    sb_offset,
    delta_query_w,
    delta_key_w,
    delta_value_w,
    decay_w,
    write_w,
    write_bias,
    decay_log_scale,
    decay_shift,
    head_gain,
    sb_out_w,
    delta_out_w,
):
    z, y, fs, tp = lax.axis_index(Z), lax.axis_index("y"), lax.axis_index("fs"), lax.axis_index("tp")
    x = hidden_in.reshape(256, 1024)

    across = functools.partial(lax.ppermute, axis_name="tp", perm=[(0, 1), (1, 0)])
    swap = lambda v: across(v)
    right, left = ring(Z, 8, 1), ring(Z, 8, 7)
    around = lambda axis, v: [v] + [ring(axis, 4, d)(v) for d in (1, 2, 3)]
    pick = lambda w, at, n: lax.dynamic_slice_in_dim(w, at, n, 1)
    item = lambda v, at: lax.dynamic_index_in_dim(v, at, 0, keepdims=False)

    mine = jnp.concatenate(
        [pick(sb_query_w, z * 64, 64), jnp.zeros((512, 64), bf16), pick(sb_key_w, z * 64, 64), pick(sb_value_w, z * 64, 64)]
        + [pick(w, y * 128, 128) for w in (delta_query_w, delta_key_w, delta_value_w)],
        axis=1,
    )
    r1, l1 = right(x), left(x)
    at_y = around("y", x)
    weights = around("fs", mine)
    r2, l2 = right(r1), left(l1)
    r3, l3 = right(r2), left(l2)
    r4, l4 = right(r3[:128]), left(l3[128:])
    other_y = [swap(v) for v in at_y]
    other_r = [swap(v) for v in (r1, r2, r3, r4)]
    other_l = [swap(v) for v in (l1, l2, l3, l4)]
    shifts = around("y", decay_shift.reshape(4, 256))

    place = jnp.stack([y, fs, tp, z]).astype(jnp.int32)
    q, kv = stick_project(
        place,
        weights,
        [x, r1, l1, r2, l2, r3, l3, r4, l4],
        [other_y[0]] + [v for pair in zip(other_r, other_l) for v in pair],
    )
    kvs = around("y", kv)
    qf, of, end = delta_local(
        place, decay_log_scale, write_bias, decay_w.T, write_w.T, weights, at_y, other_y, shifts
    )
    ends = lax.all_to_all(jnp.broadcast_to(end[None], (8, 128, 256)), Z, 0, 0, tiled=True)
    dm = delta_finish(head_gain.reshape(1, 128), place, qf, of, ends)
    dm = lax.all_to_all(dm.reshape(8, 128, 128), ("y", "tp"), 0, 0, tiled=True)
    outs_other = [swap(sb_out_w), swap(delta_out_w)]

    u = jnp.asarray(np.tril(np.ones((CH, CH), np.float32), -1), bf16)
    table = item(jnp.asarray(work_list()), 4 * z + y)
    sb = stick_attention(table, sb_offset, q, u, kvs)
    sb = lax.all_to_all(sb, (*Z, "tp"), 0, 0, tiled=True)

    sb = sb.reshape(8, 2, 64, 2, 64).transpose(1, 3, 2, 0, 4).reshape(2, 128, 512)
    dm = dm.reshape(4, 2, 128, 128).transpose(1, 2, 0, 3).reshape(2, 128, 512)

    def out_rows(rows, own_w, other_w):
        return jnp.dot(item(rows, tp), own_w, preferred_element_type=f32) + jnp.dot(
            item(rows, 1 - tp), other_w, preferred_element_type=f32
        )

    out = out_rows(dm, delta_out_w, outs_other[1])
    out = out + out_rows(sb, sb_out_w, outs_other[0])
    return out.astype(bf16).reshape(1, 128, 2048)


def solution(mesh):
    finer = Mesh(mesh.devices.reshape(2, 4, 4, mesh.shape["fs"], mesh.shape["tp"]), AXES)
    sp = ("zh", "zl", "y")
    return jax.shard_map(
        on_device,
        mesh=finer,
        in_specs=(
            P("fs", sp, "tp"),
            P("fs", "tp"),
            P("fs", "tp"),
            P("fs", "tp"),
            P("tp"),
            P("fs", "tp"),
            P("fs", "tp"),
            P("fs", "tp"),
            P(None, "tp"),
            P(None, "tp"),
            P("tp"),
            P("tp"),
            P("fs", "tp", sp),
            P(),
            P("tp", None),
            P("tp", None),
        ),
        out_specs=P("fs", (*sp, "tp"), None),
        check_vma=False,
    )
```

```python
import functools

import jax
import jax.numpy as jnp
import numpy as np
from jax import lax
from jax.experimental import pallas as pl
from jax.experimental.pallas import tpu as pltpu
from jax.sharding import Mesh
from jax.sharding import PartitionSpec as P


f32 = jnp.float32
bf16 = jnp.bfloat16
LOG2E = float(np.log2(np.e))
EPS = 1e-6
CH = 256
NT = (((1,), (1,)), ((), ()))
Z = ("zh", "zl")
AXES = ("zh", "zl", "y", "fs", "tp")


SLOT = (0, 2, 4, 6, 7, 5, 3, 1)
PAIRS, SINGLE, SLOTS, COUNT, HEAD = 0, 256, 320, 328, 329


def work_list():
    table = np.zeros((32, 384), np.int32)
    for z in range(8):
        slot = lambda i: SLOT[(i - z) % 8]
        for y in range(4):
            row = table[4 * z + y]
            place = lambda i, m: (m % 4) * 8 + slot((4 * i + y - m) // 4)
            steps = [(slot(2 * p), slot(2 * p + 1), place(2 * p, m)) for p in (3, 2, 1, 0) for m in range(1, 8 * p + y + 1)]
            for n, step in enumerate(steps):
                for k in range(3):
                    row[PAIRS + 64 * k + n] = step[k]
            for chain, ps in enumerate(((3, 1), (2, 0))):
                steps_one = [(slot(2 * p + 1), place(2 * p + 1, m)) for p in ps for m in range(1, 5)]
                for n, step in enumerate(steps_one):
                    row[SINGLE + 16 * chain + n] = step[0]
                    row[SINGLE + 16 * chain + 8 + n] = step[1]
            row[SLOTS : SLOTS + 8] = [slot(i) for i in range(8)]
            row[COUNT], row[HEAD] = len(steps), z
    return table


def stick_kernel(table, off_ref, q, u_ref, *refs):
    kv_refs, o_ref, (acc, run, kvs, kt, late_a, late_b, sp_a, sp_b) = refs[:4], refs[4], refs[5:]
    off = off_ref[table[HEAD]] * LOG2E
    for d in range(4):
        for n in range(8):
            block = kv_refs[d][n]
            kvs[d * 8 + n] = block
            kt[d * 8 + n] = jnp.transpose(block)

    def tile(slots, c, masked):
        size = CH * len(slots)
        join = lambda ref: jnp.concatenate([ref[s] for s in slots], axis=0) if len(slots) > 1 else ref[slots[0]]
        kv = kvs[c]
        z = jnp.dot(join(q), kt[c], preferred_element_type=f32) * (0.125 * LOG2E) + off
        sp = jnp.maximum(jnp.log2(1.0 + jnp.exp2(jnp.minimum(z, 40.0))), z)
        if masked:
            shape = (size, CH)
            seen = lax.broadcasted_iota(jnp.int32, shape, 1) < lax.broadcasted_iota(jnp.int32, shape, 0)
            sp = jnp.where(seen, sp, 0.0)
        after = jnp.dot(sp.astype(bf16), u_ref[...], preferred_element_type=f32)
        total = after[:, :1] + sp[:, :1]
        if masked:
            w = jnp.where(seen, jnp.exp2((z - sp) - after), 0.0)
            total = jnp.broadcast_to(total, (size, 128))
            out = jnp.dot(w.astype(bf16), kv, preferred_element_type=f32)
        else:
            r = join(run)
            w = jnp.exp2((z - sp) - (after + jnp.concatenate([r, r], axis=1)))
            total = r + total
            out = join(acc) + jnp.dot(w.astype(bf16), kv, preferred_element_type=f32)
        for k, s in enumerate(slots):
            run[s] = total[k * CH : k * CH + CH]
            acc[s] = out[k * CH : k * CH + CH]

    def diagonal(n, carry):
        for k in range(2):
            tile((2 * n + k,), 2 * n + k, True)
        return carry

    lax.fori_loop(0, 4, diagonal, 0)

    def pair_step(n):
        c = table[PAIRS + 128 + n]
        return (table[PAIRS + n], table[PAIRS + 64 + n]), (c,)

    def single_step(n):
        n = lax.rem(n, 8)
        at = (SINGLE + n, SINGLE + 16 + n)
        return tuple(table[k] for k in at), tuple(table[k + 8] for k in at)

    def product(rows, columns, keys):
        if len(keys) == 1:
            return jnp.dot(jnp.concatenate(rows), columns[keys[0]], preferred_element_type=f32)
        return jnp.concatenate([jnp.dot(r, columns[c], preferred_element_type=f32) for r, c in zip(rows, keys)])

    def scores(step, late, sp_at):
        slots, keys = step
        z = product([q[s] for s in slots], kt, keys) * (0.125 * LOG2E) + off
        sp = jnp.maximum(jnp.log2(1.0 + jnp.exp2(jnp.minimum(z, 40.0))), z)
        late[...] = z - sp
        sp_at[...] = sp.astype(bf16)

    def weigh(step, late, sp_at):
        slots, keys = step
        after = jnp.dot(sp_at[...], u_ref[...], preferred_element_type=f32)
        r = jnp.concatenate([run[s] for s in slots])
        w = jnp.exp2(late[...] - (after + jnp.concatenate([r, r], axis=1))).astype(bf16)
        out = product([w[:CH], w[CH:]], kvs, keys)
        total = r + (after[:, :1] + sp_at[:, :1].astype(f32))
        for k, s in enumerate(slots):
            rows = slice(k * CH, k * CH + CH)
            run[s] = total[rows]
            acc[s] += out[rows]

    def sweep(step, pairs_of_steps):
        scores(step(0), late_a, sp_a)

        def two(m, carry):
            weigh(step(2 * m), late_a, sp_a)
            scores(step(2 * m + 1), late_b, sp_b)
            weigh(step(2 * m + 1), late_b, sp_b)
            scores(step(2 * m + 2), late_a, sp_a)
            return carry

        lax.fori_loop(0, pairs_of_steps, two, 0)

    sweep(single_step, 4)
    sweep(pair_step, table[COUNT] // 2)
    lane = lax.broadcasted_iota(jnp.int32, (64, 128), 1)
    for i in range(8):
        rows = acc[table[SLOTS + i]]
        for h in range(2):
            low, high = rows[128 * h : 128 * h + 64], rows[128 * h + 64 : 128 * h + 128]
            o_ref[2 * i + h] = jnp.where(lane < 64, pltpu.roll(low, 64, 1), high).astype(bf16)


def stick_attention(table, off, q, u, kvs):
    smem = pl.BlockSpec(memory_space=pltpu.SMEM)
    vmem = pl.BlockSpec(memory_space=pltpu.VMEM)
    return pl.pallas_call(
        stick_kernel,
        out_shape=jax.ShapeDtypeStruct((16, 64, 128), bf16),
        in_specs=[smem] * 2 + [vmem] * 6,
        out_specs=vmem,
        scratch_shapes=[
            pltpu.VMEM((8, CH, 128), f32),
            pltpu.VMEM((8, CH, 128), f32),
            pltpu.VMEM((32, CH, 128), bf16),
            pltpu.VMEM((32, 128, CH), bf16),
            pltpu.VMEM((2 * CH, CH), f32),
            pltpu.VMEM((2 * CH, CH), f32),
            pltpu.VMEM((2 * CH, CH), bf16),
            pltpu.VMEM((2 * CH, CH), bf16),
        ],
        cost_estimate=pl.CostEstimate(flops=20_000_000_000, bytes_accessed=4_000_000, transcendentals=26_000_000),
        name="stick_attention",
    )(table, off, q, u, *kvs)


def fetch(own, other, x_all, sems):
    copies = []
    for h, pieces in enumerate((own, other)):
        at = 0
        for k, piece in enumerate(pieces):
            rows = piece.shape[0]
            to = x_all.at[at // CH, pl.ds(at % CH, rows), pl.ds(h * 1024, 1024)]
            copy = pltpu.make_async_copy(piece, to, sems.at[h, k])
            copy.start()
            copies.append(copy)
            at += rows
    return copies


def project_rows(w_copies, copies, one, x_all, sems, w_ref, q_ref, kv_ref):
    for copy in w_copies:
        copy.wait()
    halves = len(copies) // 2

    def chunk(n):
        out = jnp.dot(x_all[n], w_ref[...], preferred_element_type=f32).astype(bf16)
        q_ref[n] = out[:, :128]
        kv_ref[n] = out[:, 128:]

    def whole(n, carry):
        for h in range(2):
            pltpu.make_async_copy(one, x_all.at[n, :, pl.ds(h * 1024, 1024)], sems.at[h, n]).wait()
        chunk(n)
        return carry

    lax.fori_loop(0, 7, whole, 0)
    for k in (7, 8, halves + 7, halves + 8):
        copies[k].wait()
    chunk(7)


def fetch_weights(place, pieces, columns, w_all, sems):
    copies = []
    for d, piece in enumerate(pieces):
        at = lax.rem(place[1] - d - 2 * place[2] + 8, 4)
        to = w_all.at[pl.ds(pl.multiple_of(at * 512, 512), 512), :]
        copy = pltpu.make_async_copy(piece.at[:, columns], to, sems.at[d])
        copy.start()
        copies.append(copy)
    return copies


def project_kernel(place, *refs):
    weights, x, (q_ref, kv_ref, w_all, x_all, sems, w_sems) = refs[:4], refs[4:-6], refs[-6:]
    half = len(x) // 2
    w_copies = fetch_weights(place, weights, pl.ds(0, 256), w_all, w_sems)
    copies = fetch(x[:half], x[half:], x_all, sems)
    project_rows(w_copies, copies, x[0], x_all, sems, w_all, q_ref, kv_ref)


def stick_project(place, weights, own, other):
    vmem = pl.BlockSpec(memory_space=pltpu.VMEM)
    anywhere = pl.BlockSpec(memory_space=pl.ANY)
    shape = jax.ShapeDtypeStruct((8, CH, 128), bf16)
    return pl.pallas_call(
        project_kernel,
        out_shape=(shape, shape),
        in_specs=[pl.BlockSpec(memory_space=pltpu.SMEM)] + [anywhere] * (4 + len(own) + len(other)),
        out_specs=(vmem, vmem),
        scratch_shapes=[
            pltpu.VMEM((2048, 256), bf16),
            pltpu.VMEM((8, CH, 2048), bf16),
            pltpu.SemaphoreType.DMA((2, len(own))),
            pltpu.SemaphoreType.DMA((4,)),
        ],
        cost_estimate=pl.CostEstimate(flops=2_200_000_000, bytes_accessed=10_000_000, transcendentals=0),
        name="stick_project",
    )(place, *weights, *own, *other)


def mm(a, b, dims=(((1,), (0,)), ((), ()))):
    return lax.dot_general(a.astype(bf16), b.astype(bf16), dims, preferred_element_type=f32)


def silu(u):
    return u * jax.nn.sigmoid(u)


def unit(u):
    return u * lax.rsqrt(jnp.sum(u * u, axis=-1, keepdims=True) + EPS)


def delta_kernel(place, scale_ref, bias_ref, decay_ref, write_ref, *refs):
    shifts, weights, own, other = refs[:4], refs[4:8], refs[8:12], refs[12:16]
    qf_ref, of_ref, end_ref, x_all, w_all, side_w, proj_all, maps, addend, rows_all, sems, w_sems = refs[16:]
    y, tp = place[0], place[2]
    w_copies = fetch_weights(place, weights, pl.ds(256, 384), w_all, w_sems)
    fetch(own, other, x_all, sems)
    minus_scale = -jnp.exp(jnp.full((CH, 1), scale_ref[y], f32))
    bias = bias_ref[y]
    for h in range(2):
        at = pl.ds(pl.multiple_of((tp if h == 0 else 1 - tp) * 1024, 1024), 1024)
        side_w[:, h * 1024 : h * 1024 + 1024] = jnp.concatenate([decay_ref[:, at], write_ref[:, at]], axis=0)
    lanes = lax.broadcasted_iota(jnp.int32, (CH, 128), 1)
    for d in range(4):
        proj_all[lax.rem(y - d + 4, 4), :, 384:] = jnp.transpose(jnp.broadcast_to(shifts[d][pl.ds(y, 1), :], (128, CH)))
    for copy in w_copies:
        copy.wait()
    narrow = lax.broadcasted_iota(jnp.int32, (CH, 8), 1)

    def project(d, carry):
        for h in range(2):
            pltpu.make_async_copy(own[0], x_all.at[d, :, pl.ds(h * 1024, 1024)], sems.at[h, d]).wait()
        x = x_all[d]
        at = lax.rem(y - d + 4, 4)
        proj_all[at, :, :384] = jnp.dot(x, w_all[...], preferred_element_type=f32)
        pre = lax.dot_general(x, side_w[...], NT, preferred_element_type=f32)
        decay_pre = jnp.sum(jnp.where(narrow == y, pre, 0.0), axis=1, keepdims=True)
        write_pre = jnp.sum(jnp.where(narrow == y + 4, pre, 0.0), axis=1, keepdims=True)
        proj_all[at, :, 384:] = jnp.where(lanes == 0, decay_pre, jnp.where(lanes == 1, write_pre, proj_all[at, :, 384:]))
        return carry

    lax.fori_loop(0, 4, project, 0)
    span = (CH, CH)
    row = lax.broadcasted_iota(jnp.int32, span, 0)
    col = lax.broadcasted_iota(jnp.int32, span, 1)
    same = (row // 64) == (col // 64)
    inclusive = jnp.logical_and(same, col <= row)
    strict = jnp.logical_and(same, col < row)
    sums = jnp.concatenate([jnp.where(inclusive, 1.0, 0.0), jnp.where(same, 1.0, 0.0)], axis=0)
    eye = jnp.where(row == col, 1.0, 0.0)
    wide = lax.broadcasted_iota(jnp.int32, (128, CH), 1) // 64
    small_eye = jnp.where(
        lax.broadcasted_iota(jnp.int32, (128, 128), 0) == lax.broadcasted_iota(jnp.int32, (128, 128), 1), 1.0, 0.0
    )

    def blocks(m, carry):
        tiles = range(2)
        cum, tot, q, k, v, beta = [], [], [], [], [], []
        for t in tiles:
            proj = proj_all[2 * m + t]
            dq, dk, dv = (proj[:, 128 * n : 128 * n + 128].astype(bf16).astype(f32) for n in range(3))
            pre = proj[:, 384:385]
            softplus = jnp.maximum(pre, 0.0) + jnp.log1p(jnp.exp(-jnp.abs(pre)))
            g = minus_scale * softplus + proj[:, 386:387]
            beta.append(jax.nn.sigmoid(proj[:, 385:386] + bias))
            q.append(unit(silu(dq)) * 128**-0.5)
            k.append(unit(silu(dk)))
            v.append(silu(dv))
            g1 = g.astype(bf16).astype(f32)
            g2 = (g - g1).astype(bf16).astype(f32)
            g3 = g - g1 - g2
            parts = jnp.where(lanes == 0, g1, jnp.where(lanes == 1, g2, jnp.where(lanes == 2, g3, 0.0)))
            s = mm(sums, parts)
            s = jnp.broadcast_to(s[:, 0:1] + s[:, 1:2] + s[:, 2:3], (2 * CH, 128))
            cum.append(s[:CH])
            tot.append(s[CH:])
        table = []
        for t in tiles:
            across = jnp.transpose(cum[t])[0:1, :]
            spread = cum[t][:, 0:1] - across
            table.append(jnp.where(inclusive, jnp.exp(jnp.where(inclusive, spread, 0.0)), 0.0))
        keys_beta = [k[t] * beta[t] for t in tiles]
        power = [jnp.where(strict, mm(keys_beta[t], k[t], NT) * table[t], 0.0) for t in tiles]
        inside = [mm(q[t], k[t], NT) * table[t] for t in tiles]
        inverse = [eye - power[t] for t in tiles]
        for _ in range(5):
            power = [mm(power[t], power[t]) for t in tiles]
            inverse = [inverse[t] + mm(inverse[t], power[t]) for t in tiles]
        growth = [jnp.exp(cum[t]) for t in tiles]
        both = [
            mm(inverse[t], jnp.concatenate([keys_beta[t] * growth[t], v[t] * beta[t]], axis=1)) for t in tiles
        ]
        seen = [mm(inside[t], both[t]) for t in tiles]
        for t in tiles:
            n0 = 4 * (2 * m + t)
            reach = q[t] * growth[t] - seen[t][:, :128]
            damped = jnp.transpose(k[t] * jnp.exp(tot[t] - cum[t]))
            moved = mm(jnp.concatenate([jnp.where(wide == b, damped, 0.0) for b in range(4)], axis=0), both[t])
            for b in range(4):
                decay = jnp.exp(tot[t][b * 64 : b * 64 + 1, :])
                piece = moved[b * 128 : b * 128 + 128]
                maps[n0 + b, :64] = reach[b * 64 : b * 64 + 64].astype(bf16)
                maps[n0 + b, 64:] = (small_eye * decay - piece[:, :128]).astype(bf16)
                addend[n0 + b, :64] = seen[t][b * 64 : b * 64 + 64, 128:]
                addend[n0 + b, 64:] = piece[:, 128:]
        return carry

    lax.fori_loop(0, 2, blocks, 0)
    rows_all[...] = jnp.concatenate([small_eye, jnp.zeros((128, 128), f32)], axis=1)

    def chain(n, carry):
        moved = jnp.dot(maps[n], rows_all[...].astype(bf16), preferred_element_type=f32)
        after = moved[:, 128:] + addend[n]
        at = pl.ds(pl.multiple_of(n * 64, 64), 64)
        qf_ref[at, :] = moved[:64, :128]
        of_ref[at, :] = after[:64]
        rows_all[...] = jnp.concatenate([moved[64:, :128], after[64:]], axis=1)
        return carry

    lax.fori_loop(0, 16, chain, 0)
    end_ref[...] = rows_all[...].astype(bf16)


def delta_local(place, scale, bias, decay_w, write_w, weights, own, other, shifts):
    smem = pl.BlockSpec(memory_space=pltpu.SMEM)
    vmem = pl.BlockSpec(memory_space=pltpu.VMEM)
    return pl.pallas_call(
        delta_kernel,
        out_shape=(
            jax.ShapeDtypeStruct((1024, 128), f32),
            jax.ShapeDtypeStruct((1024, 128), f32),
            jax.ShapeDtypeStruct((128, 256), bf16),
        ),
        in_specs=[smem] * 3 + [vmem] * 6 + [pl.BlockSpec(memory_space=pl.ANY)] * 12,
        out_specs=(vmem,) * 3,
        scratch_shapes=[
            pltpu.VMEM((4, CH, 2048), bf16),
            pltpu.VMEM((2048, 384), bf16),
            pltpu.VMEM((8, 2048), bf16),
            pltpu.VMEM((4, CH, 512), f32),
            pltpu.VMEM((16, 192, 128), bf16),
            pltpu.VMEM((16, 192, 128), f32),
            pltpu.VMEM((128, 256), f32),
            pltpu.SemaphoreType.DMA((2, 4)),
            pltpu.SemaphoreType.DMA((4,)),
        ],
        cost_estimate=pl.CostEstimate(flops=12_000_000_000, bytes_accessed=8_000_000, transcendentals=1_000_000),
        name="delta_local",
    )(place, scale, bias, decay_w, write_w, *shifts, *weights, *own, *other)


def finish_kernel(gain_ref, qf_ref, of_ref, *refs):
    maps, o_ref = refs[:-1], refs[-1]
    state = jnp.zeros((128, 128), f32)
    for ref in maps:
        state = mm(ref[:, :128], state) + ref[:, 128:].astype(f32)
    for t in range(4):
        rows = slice(t * CH, (t + 1) * CH)
        o = mm(qf_ref[rows, :], state) + of_ref[rows, :]
        o = o * lax.rsqrt(jnp.mean(o * o, axis=-1, keepdims=True) + EPS) * gain_ref[...]
        o_ref[rows, :] = o.astype(bf16)


def delta_finish(gain, qf, of, maps):
    vmem = pl.BlockSpec(memory_space=pltpu.VMEM)
    return pl.pallas_call(
        finish_kernel,
        out_shape=jax.ShapeDtypeStruct((1024, 128), bf16),
        in_specs=[vmem] * (3 + len(maps)),
        out_specs=vmem,
        cost_estimate=pl.CostEstimate(flops=1_000_000_000, bytes_accessed=2_000_000, transcendentals=2_000),
        name="delta_finish",
    )(gain, qf, of, *maps)


def ring(axis, size, step):
    return functools.partial(lax.ppermute, axis_name=axis, perm=[(i, (i + step) % size) for i in range(size)])


def on_device(
    hidden_in,
    sb_query_w,
    sb_key_w,
    sb_value_w,
    sb_offset,
    delta_query_w,
    delta_key_w,
    delta_value_w,
    decay_w,
    write_w,
    write_bias,
    decay_log_scale,
    decay_shift,
    head_gain,
    sb_out_w,
    delta_out_w,
):
    z, y, fs, tp = lax.axis_index(Z), lax.axis_index("y"), lax.axis_index("fs"), lax.axis_index("tp")
    x = hidden_in.reshape(256, 1024)

    across = functools.partial(lax.ppermute, axis_name="tp", perm=[(0, 1), (1, 0)])
    swap = lambda v: across(v)
    right, left = ring(Z, 8, 1), ring(Z, 8, 7)
    around = lambda axis, v: [v] + [ring(axis, 4, d)(v) for d in (1, 2, 3)]
    pick = lambda w, at, n: lax.dynamic_slice_in_dim(w, at, n, 1)
    item = lambda v, at: lax.dynamic_index_in_dim(v, at, 0, keepdims=False)

    mine = jnp.concatenate(
        [pick(sb_query_w, z * 64, 64), jnp.zeros((512, 64), bf16), pick(sb_key_w, z * 64, 64), pick(sb_value_w, z * 64, 64)]
        + [pick(w, y * 128, 128) for w in (delta_query_w, delta_key_w, delta_value_w)],
        axis=1,
    )
    r1, l1 = right(x), left(x)
    at_y = around("y", x)
    weights = around("fs", mine)
    r2, l2 = right(r1), left(l1)
    r3, l3 = right(r2), left(l2)
    r4, l4 = right(r3[:128]), left(l3[128:])
    other_y = [swap(v) for v in at_y]
    other_r = [swap(v) for v in (r1, r2, r3, r4)]
    other_l = [swap(v) for v in (l1, l2, l3, l4)]
    shifts = around("y", decay_shift.reshape(4, 256))

    place = jnp.stack([y, fs, tp]).astype(jnp.int32)
    q, kv = stick_project(
        place,
        weights,
        [x, r1, l1, r2, l2, r3, l3, r4, l4],
        [other_y[0]] + [v for pair in zip(other_r, other_l) for v in pair],
    )
    kvs = around("y", kv)
    qf, of, end = delta_local(
        place, decay_log_scale, write_bias, decay_w.T, write_w.T, weights, at_y, other_y, shifts
    )
    ends = [
        functools.partial(lax.ppermute, axis_name=Z, perm=[(i, i + d) for i in range(8 - d)])(end)
        for d in range(7, 0, -1)
    ]
    dm = delta_finish(head_gain.reshape(1, 128), qf, of, ends)
    dm = lax.all_to_all(dm.reshape(8, 128, 128), ("y", "tp"), 0, 0, tiled=True)
    outs_other = [swap(sb_out_w), swap(delta_out_w)]

    u = jnp.asarray(np.tril(np.ones((CH, CH), np.float32), -1), bf16)
    table = item(jnp.asarray(work_list()), 4 * z + y)
    sb = stick_attention(table, sb_offset, q, u, kvs)
    sb = lax.all_to_all(sb, (*Z, "tp"), 0, 0, tiled=True)

    sb = sb.reshape(8, 2, 64, 2, 64).transpose(1, 3, 2, 0, 4).reshape(2, 128, 512)
    dm = dm.reshape(4, 2, 128, 128).transpose(1, 2, 0, 3).reshape(2, 128, 512)

    def out_rows(rows, own_w, other_w):
        return jnp.dot(item(rows, tp), own_w, preferred_element_type=f32) + jnp.dot(
            item(rows, 1 - tp), other_w, preferred_element_type=f32
        )

    out = out_rows(dm, delta_out_w, outs_other[1])
    out = out + out_rows(sb, sb_out_w, outs_other[0])
    return out.astype(bf16).reshape(1, 128, 2048)


def solution(mesh):
    finer = Mesh(mesh.devices.reshape(2, 4, 4, mesh.shape["fs"], mesh.shape["tp"]), AXES)
    sp = ("zh", "zl", "y")
    return jax.shard_map(
        on_device,
        mesh=finer,
        in_specs=(
            P("fs", sp, "tp"),
            P("fs", "tp"),
            P("fs", "tp"),
            P("fs", "tp"),
            P("tp"),
            P("fs", "tp"),
            P("fs", "tp"),
            P("fs", "tp"),
            P(None, "tp"),
            P(None, "tp"),
            P("tp"),
            P("tp"),
            P("fs", "tp", sp),
            P(),
            P("tp", None),
            P("tp", None),
        ),
        out_specs=P("fs", (*sp, "tp"), None),
        check_vma=False,
    )
```
